512 devices in a mesh: ep: 128 (over z, x, core), tp: 4 (over y).
Axes of the slice: x: 4, y: 4, z: 16, core: 2. Of those that a mesh axis runs over, the one named last changes fastest.
Arguments:
- tokens: bfloat16 [16384, 2048], P('ep'), may hold values from -6 to 6
- norm_gain: float32 [2048], replicated, may hold values from 0.1 to 1.9
- expert_ids: int32 [16384, 2], P('ep'), may hold values from 0 to 31, all different within a row; in each aligned block of 128 rows (0 to 127, 128 to 255, ...) at most 12 rows name the same one
- gate_weights: float32 [16384, 2], P('ep'), may hold values from 0.2 to 1
- w_gate: bfloat16 [2048, 131072], P(None, ('ep', 'tp')), may hold values from -0.125 to 0.125
- w_up: bfloat16 [2048, 131072], P(None, ('ep', 'tp')), may hold values from -0.125 to 0.125
- w_down: bfloat16 [131072, 2048], P('ep', 'tp'), may hold values from -0.09375 to 0.09375
Outputs:
- moe_out: bfloat16 [16384, 2048], P('ep', 'tp')
The draws below stay inside these ranges and needn't reach their ends.
Inputs may be any that keep to these rules, and one draw needn't show every extreme that they name: `expert_ids`: each token names 2 different experts; in each aligned block of 128 rows no expert is named by more than 12 rows, a bound that some block reaches.
All inputs are finite; a program needn't handle non-finite values.
Results may differ from the reference program's by a relative error of at most 0.0071.
Values may be sent and summed in bfloat16 or wider, within the bound.
No kernel may reach another device: no remote copies, remote signals or barrier semaphores. Data moves between devices by JAX's collectives and lax.ppermute only.
A program may use at most 64 MiB of HBM per device.

```python
import math
import jax
import jax.numpy as jnp
import numpy as np
from jax import lax

D = 2048
FF = 4096
TOP = 2
TOK_DEV = 128
GROUP = 4
EXPERTS = 32
CAP = 12
TOKENS = 16384
N_EP = 128


def levels(own_key, shape, pieces, smallest, largest):
    level = 1.0
    for axis_at, parts in pieces:
        heights = jax.random.uniform(jax.random.fold_in(jax.random.fold_in(own_key, 6), axis_at), (parts,), jnp.float32, smallest / len(pieces), largest / len(pieces))
        level = level * jnp.repeat(jnp.exp(heights), shape[axis_at] // parts).reshape((-1,) + (1,) * (len(shape) - 1 - axis_at))
    return level


def assign_block(key, own, number, rows, count, top, reach, slope):
    order = jax.random.permutation(key, count)
    packed, ordinary = load_shares(count, rows * top, reach, slope, True), load_shares(count, rows * top, reach, slope, False)
    places = jnp.arange(count)

    def named(lengths, rotation):
        used = int((lengths > 0).sum())
        fixed = max(1, used // 4)
        moved = fixed + (places - fixed + rotation * (used - fixed)) % max(1, count - fixed)
        return jnp.zeros((count,), jnp.int32).at[order[jnp.where(places < fixed, places, moved)]].set(jnp.asarray(lengths, jnp.int32))

    lengths = jnp.where(number % 4 == 0, named(packed, number // 4), named(ordinary, number - number // 4 - 1))
    mixed = jax.random.permutation(jax.random.fold_in(own, 3), count)
    giver, receiver = mixed[0:count // 2 * 2:2], mixed[1:count // 2 * 2:2]
    margin = jnp.minimum(lengths[giver] - 1, reach - lengths[receiver]) // 2
    margin = jnp.where((giver == order[0]) | (receiver == order[0]) | (lengths[receiver] == 0), 0, jnp.maximum(margin, 0))
    moved = jax.random.randint(jax.random.fold_in(own, 4), (count // 2,), 0, 1 << 20) % (margin + 1)
    lengths = lengths.at[giver].add(-moved).at[receiver].add(moved)
    items = jnp.searchsorted(jnp.cumsum(lengths), jnp.arange(rows * top), side="right").astype(jnp.int32)
    table = items.reshape(top, rows).T
    table = table[jax.random.permutation(jax.random.fold_in(own, 1), rows)]
    rotation = jax.random.randint(jax.random.fold_in(own, 2), (rows, 1), 0, top)
    return jnp.take_along_axis(table, (jnp.arange(top)[None, :] + rotation) % top, axis=1)


def load_shares(number_of, total, limit, skew, full):
    loads = [(1 << 20) // math.isqrt(grade ** skew) + 1 for grade in range(1, number_of + 1)]
    largest = limit if full else min(limit, max(-(-total // number_of), total * loads[0] // sum(loads)))
    least = 1 if total - largest >= number_of - 1 else 0
    counts, rest = [largest] + [least] * (number_of - 1), total - largest - least * (number_of - 1)
    while rest > 0:
        free = [i for i in range(1, number_of) if counts[i] < largest] or [i for i in range(1, number_of) if counts[i] < limit]
        mass, remaining = sum([loads[i] for i in free]), rest
        for i in free:
            more = min(limit - counts[i], max(1, remaining * loads[i] // mass), rest)
            counts[i] = counts[i] + more
            rest = rest - more
    return np.array(counts)


def noise(own_key, shape, deviation, limit, cuts=(), held_as=jnp.bfloat16):
    values = deviation * jax.random.normal(own_key, shape, jnp.float32)
    if cuts:
        values = values * levels(own_key, shape, cuts, -0.22, 0.18)
    return jnp.clip(values, -limit, limit).astype(held_as)


def setup_inputs(seed: int = 0) -> dict:
    key_of = jax.random.split(jax.random.key(seed), 8)
    tokens = noise(key_of[0], (TOKENS, D), 1.0, 6.0, ((0, 128),))
    norm_gain = jnp.clip(1.0 + 0.18 * jax.random.normal(key_of[1], (D,), jnp.float32), 0.1, 1.9)
    expert_ids_keys = jax.random.split(jax.random.fold_in(key_of[2], 1), TOKENS // TOK_DEV)
    expert_ids_turns = jax.random.permutation(jax.random.fold_in(key_of[2], 3), TOKENS // TOK_DEV)
    expert_ids = jax.vmap(lambda own, number: assign_block(jax.random.fold_in(key_of[2], 2), own, number, TOK_DEV, EXPERTS, TOP, CAP, 2))(expert_ids_keys, expert_ids_turns).reshape((TOKENS, TOP))
    gate_weights = jnp.clip(0.2 + 0.8 * jax.random.uniform(key_of[3], (TOKENS, TOP), jnp.float32) ** levels(key_of[3], (TOKENS, TOP), ((0, 128),), -0.2, 0.2), 0.2, 1.0)
    w_gate = noise(key_of[4], (D, EXPERTS * FF), D ** -0.5, 0.125, ((1, 512),))
    w_up = noise(key_of[5], (D, EXPERTS * FF), D ** -0.5, 0.125, ((1, 512),))
    w_down = noise(key_of[6], (EXPERTS * FF, D), FF ** -0.5, 0.09375, ((0, 128), (1, 4)))
    return {"tokens": tokens, "norm_gain": norm_gain, "expert_ids": expert_ids, "gate_weights": gate_weights, "w_gate": w_gate, "w_up": w_up, "w_down": w_down}


EPS = 1e-06

def rms_rows(values, gain):
    widened = values.astype(jnp.float32)
    scale = lax.rsqrt(lax.optimization_barrier(jnp.mean(widened * widened, axis=-1, keepdims=True)) + EPS)
    return (widened * scale * gain).astype(jnp.bfloat16)

def reference(tokens, norm_gain, expert_ids, gate_weights, w_gate, w_up, w_down):
    normed = rms_rows(tokens, norm_gain)
    block_width = FF // GROUP
    slots_most = min(CAP * N_EP, TOKENS)
    flat_ids = expert_ids.reshape(-1).astype(jnp.int32)
    flat_gates = gate_weights.reshape(-1).astype(jnp.float32)
    owners = (jnp.arange(TOKENS * TOP, dtype=jnp.int32) // TOP).astype(jnp.int32)

    def one_expert(expert, output):
        matches = (flat_ids == expert).astype(jnp.int32)
        ranks = (jnp.cumsum(matches) - matches).astype(jnp.int32)
        target = jnp.where(matches == 1, ranks, slots_most).astype(jnp.int32)
        sources = jnp.zeros((slots_most,), jnp.int32).at[target].set(owners, mode='drop')
        scales = jnp.zeros((slots_most,), jnp.float32).at[target].set(flat_gates, mode='drop')
        picked = normed[sources]
        gate_cols = lax.dynamic_slice_in_dim(w_gate, expert * FF, FF, 1)
        up_cols = lax.dynamic_slice_in_dim(w_up, expert * FF, FF, 1)
        down_rows = lax.dynamic_slice_in_dim(w_down, expert * FF, FF, 0)
        gate_proj = jnp.dot(picked, gate_cols, preferred_element_type=jnp.float32)
        upper = jnp.dot(picked, up_cols, preferred_element_type=jnp.float32)
        hidden = (jax.nn.silu(gate_proj) * upper).astype(jnp.bfloat16)

        def add_block(block, total):
            piece = lax.dynamic_slice_in_dim(hidden, block * block_width, block_width, 1)
            weights = lax.dynamic_slice_in_dim(down_rows, block * block_width, block_width, 0)
            partial_out = jnp.dot(piece, weights, preferred_element_type=jnp.float32).astype(jnp.bfloat16)
            partial_out = lax.optimization_barrier(partial_out)
            return total + partial_out.astype(jnp.float32)
        total = lax.fori_loop(0, GROUP, add_block, jnp.zeros((slots_most, D), jnp.float32))
        return output.at[sources].add(total * scales[:, None])
    output = lax.fori_loop(0, EXPERTS, one_expert, jnp.zeros((TOKENS, D), jnp.float32))
    return output.astype(jnp.bfloat16)
```

```python
import jax
import jax.numpy as jnp
from jax import lax
from jax.sharding import Mesh
from jax.sharding import PartitionSpec as P

EPS = 1e-06
EP = ("z", "xh", "xl", "c")
EP_TP = ("z", "xh", "xl", "c", "y")
EXPERTS = 32
CAP = 12
RING = [(y, (y + 1) % 4) for y in range(4)] + [(4 + y, 4 + (y - 1) % 4) for y in range(4)]
SWAP = [(0, 1), (1, 0)]


def rms_rows(values, gain):
    widened = values.astype(jnp.float32)
    scale = lax.rsqrt(jnp.mean(widened * widened, axis=-1, keepdims=True) + EPS)
    return (widened * scale * gain).astype(jnp.bfloat16)


def ring(block):
    return lax.ppermute(block, ("c", "y"), RING)


def dot32(a, b):
    return jnp.dot(a, b, preferred_element_type=jnp.float32)


def spread(per_expert, width, precision=None):
    expert = lax.broadcasted_iota(jnp.int32, (EXPERTS, EXPERTS * width), 1) // width
    own = lax.broadcasted_iota(jnp.int32, (EXPERTS, EXPERTS * width), 0)
    table = (expert == own).astype(per_expert.dtype)
    return jnp.dot(per_expert, table, precision=precision, preferred_element_type=jnp.float32)


def on_device(tokens, norm_gain, expert_ids, gate_weights, w_gate, w_up, w_down):
    y = lax.axis_index("y")
    turn = 1 - 2 * lax.axis_index("c")
    rows = tokens.shape[0]
    width = tokens.shape[1]
    share = CAP // 4
    normed = rms_rows(tokens, norm_gain)
    experts = jnp.arange(EXPERTS, dtype=jnp.int32)[None, :]
    first = expert_ids[:, 0:1] == experts
    second = expert_ids[:, 1:2] == experts
    named = first | second
    weight = jnp.where(first, gate_weights[:, 0:1], 0.0) + jnp.where(
        second, gate_weights[:, 1:2], 0.0
    )
    earlier = (
        lax.broadcasted_iota(jnp.int32, (rows, rows), 0)
        > lax.broadcasted_iota(jnp.int32, (rows, rows), 1)
    ).astype(jnp.bfloat16)
    rank = dot32(earlier, named.astype(jnp.bfloat16))
    rank = jnp.where(named, rank, -1.0).astype(jnp.bfloat16)
    column = lax.broadcasted_iota(jnp.int32, (1, EXPERTS * share), 1)
    slot = share * y + column % share
    selector = (spread(rank, share) == slot.astype(jnp.float32)).astype(jnp.bfloat16)
    mine = lax.dot_general(
        selector, normed, (((0,), (0,)), ((), ())), preferred_element_type=jnp.float32
    ).astype(jnp.bfloat16)
    mine = mine.reshape(EXPERTS, share * width // 128, 128)
    arrived = lax.all_to_all(mine, ("z", "xh"), 0, 0, tiled=True)
    arrived = arrived.reshape(EXPERTS * share, width)

    other = lax.ppermute(arrived, "xl", SWAP)
    near, far = [arrived], [other]
    for _ in range(3):
        near.append(ring(near[-1]))
        far.append(ring(far[-1]))

    def hidden_of(block):
        gate_proj = dot32(block, w_gate)
        upper = dot32(block, w_up)
        return (jax.nn.silu(gate_proj) * upper).astype(jnp.bfloat16)

    own_hidden, partner_hidden = [], []
    for step in range(4):
        block = jnp.concatenate([near[step], far[step]], 0)
        swapped = lax.ppermute(block, "c", SWAP)
        own_hidden.append(hidden_of(block))
        partner_hidden.append(hidden_of(swapped))
    own = jnp.concatenate(own_hidden, 0)
    partner = jnp.concatenate(partner_hidden, 0)
    block_rows = own.shape[0] // 4
    depth = own.shape[1]
    own_sum = partner_sum = 0.0
    for step in range(4):
        start = ((y - turn * step) % 4) * depth
        down = lax.dynamic_slice_in_dim(w_down, start, depth, 0)
        own_sum += dot32(jnp.roll(own, step * block_rows, 0), down)
        partner_sum += dot32(jnp.roll(partner, -step * block_rows, 0), down)
        if step < 3:
            own, partner = ring(own), ring(partner)
    out_width = w_down.shape[1]
    pieces = (4, 2, EXPERTS * share, out_width)
    own_sum = own_sum.reshape(pieces)
    partner_sum = partner_sum.astype(jnp.bfloat16).reshape(pieces)
    away = own_sum[:, 1] + lax.ppermute(partner_sum[:, 1], "c", SWAP).astype(jnp.float32)
    back = lax.ppermute(away.astype(jnp.bfloat16), "xl", SWAP)
    home = own_sum[:, 0] + lax.ppermute(partner_sum[:, 0], "c", SWAP).astype(jnp.float32)
    home = (home + back.astype(jnp.float32)).astype(jnp.bfloat16)
    home = home.reshape(4, EXPERTS, share, out_width).transpose(1, 0, 2, 3)
    home = home.reshape(EXPERTS, CAP * out_width // 128, 128)
    returned = lax.all_to_all(home, ("z", "xh"), 0, 0, tiled=True)
    returned = returned.reshape(EXPERTS * CAP, out_width).astype(jnp.float32)
    column = lax.broadcasted_iota(jnp.int32, (1, EXPERTS * CAP), 1) % CAP
    slot = share * ((y - turn * (column // share)) % 4) + column % share
    chosen = spread(rank, CAP) == slot.astype(jnp.float32)
    spread_weight = spread(weight, CAP, lax.Precision.HIGHEST)
    combine = jnp.where(chosen, spread_weight, 0.0)
    mixed = jnp.dot(
        combine, returned, precision=lax.Precision.HIGHEST, preferred_element_type=jnp.float32
    )
    return mixed.astype(jnp.bfloat16)


def solution(mesh):
    finer = Mesh(mesh.devices.reshape(16, 2, 2, 2, 4), EP_TP)
    placed = (
        P(EP, None),
        P(),
        P(EP, None),
        P(EP, None),
        P(None, EP_TP),
        P(None, EP_TP),
        P(EP, "y"),
    )
    return jax.shard_map(
        on_device, mesh=finer, in_specs=placed, out_specs=P(EP, "y"), check_vma=False
    )
```

```python
import jax
import jax.numpy as jnp
from jax import lax
from jax.sharding import Mesh
from jax.sharding import PartitionSpec as P

EPS = 1e-06
EP = ("z", "xh", "xl", "c")
EP_TP = ("z", "xh", "xl", "c", "y")
EXPERTS = 32
CAP = 12
RING = [(y, (y + 1) % 4) for y in range(4)] + [(4 + y, 4 + (y - 1) % 4) for y in range(4)]
SWAP = [(0, 1), (1, 0)]


def rms_rows(values, gain):
    widened = values.astype(jnp.float32)
    scale = lax.rsqrt(jnp.mean(widened * widened, axis=-1, keepdims=True) + EPS)
    return (widened * scale * gain).astype(jnp.bfloat16)


def ring(block):
    return lax.ppermute(block, ("c", "y"), RING)


def dot32(a, b):
    return jnp.dot(a, b, preferred_element_type=jnp.float32)


def spread(per_expert, width, precision=None):
    expert = lax.broadcasted_iota(jnp.int32, (EXPERTS, EXPERTS * width), 1) // width
    own = lax.broadcasted_iota(jnp.int32, (EXPERTS, EXPERTS * width), 0)
    table = (expert == own).astype(per_expert.dtype)
    return jnp.dot(per_expert, table, precision=precision, preferred_element_type=jnp.float32)


def on_device(tokens, norm_gain, expert_ids, gate_weights, w_gate, w_up, w_down):
    y = lax.axis_index("y")
    turn = 1 - 2 * lax.axis_index("c")
    rows = tokens.shape[0]
    width = tokens.shape[1]
    share = CAP // 4
    block_rows = EXPERTS * share
    normed = rms_rows(tokens, norm_gain)
    experts = jnp.arange(EXPERTS, dtype=jnp.int32)[None, :]
    first = expert_ids[:, 0:1] == experts
    second = expert_ids[:, 1:2] == experts
    named = first | second
    weight = jnp.where(first, gate_weights[:, 0:1], 0.0) + jnp.where(
        second, gate_weights[:, 1:2], 0.0
    )
    earlier = (
        lax.broadcasted_iota(jnp.int32, (rows, rows), 0)
        > lax.broadcasted_iota(jnp.int32, (rows, rows), 1)
    ).astype(jnp.bfloat16)
    rank = dot32(earlier, named.astype(jnp.bfloat16))
    rank = jnp.where(named, rank, -1.0).astype(jnp.bfloat16)
    column = lax.broadcasted_iota(jnp.int32, (1, block_rows), 1)
    slot = share * y + column % share
    selector = (spread(rank, share) == slot.astype(jnp.float32)).astype(jnp.bfloat16)

    cuts = (0, width // 2, width)
    near, far = [], []
    for low, high in zip(cuts[:-1], cuts[1:]):
        mine = lax.dot_general(
            selector,
            normed[:, low:high],
            (((0,), (0,)), ((), ())),
            preferred_element_type=jnp.float32,
        ).astype(jnp.bfloat16)
        mine = mine.reshape(EXPERTS, share * (high - low) // 128, 128)
        arrived = lax.all_to_all(mine, ("z", "xh"), 0, 0, tiled=True)
        near.append(arrived.reshape(block_rows, high - low))

    gates = (w_gate, lax.ppermute(w_gate, "c", SWAP))
    uppers = (w_up, lax.ppermute(w_up, "c", SWAP))
    downs = (w_down, lax.ppermute(w_down, "c", SWAP))

    sums = [[0.0] * 4 for _ in range(4)]
    for part, (low, high) in enumerate(zip(cuts[:-1], cuts[1:])):
        block = jnp.concatenate([near[part], lax.ppermute(near[part], "xl", SWAP)], 0)
        for step in range(4):
            for i, matrix in enumerate(gates + uppers):
                sums[step][i] += dot32(block, matrix[low:high])
            if step < 3:
                block = ring(block)
    hidden = []
    for g0, g1, u0, u1 in sums:
        parts = [(jax.nn.silu(g) * u).astype(jnp.bfloat16) for g, u in ((g0, u0), (g1, u1))]
        hidden.append(jnp.concatenate(parts, 1))
    hidden = jnp.concatenate(hidden, 0)
    depth = w_gate.shape[1]
    out_width = w_down.shape[1]

    column = lax.broadcasted_iota(jnp.int32, (1, EXPERTS * CAP // 2), 1)
    spread_rank = spread(rank, CAP // 2)
    spread_weight = spread(weight, CAP // 2, lax.Precision.HIGHEST)
    mixed = 0.0
    for half in range(2):
        pieces = []
        for side in range(2):
            for q in (2 * half, 2 * half + 1):
                start = ((turn * (y - q)) & 3) * (2 * block_rows) + side * block_rows
                pieces.append(lax.dynamic_slice_in_dim(hidden, start, block_rows, 0))
        block = jnp.concatenate(pieces, 0)
        total = 0.0
        for step in range(4):
            start = ((y - turn * step) & 3) * depth
            for core in range(2):
                down = lax.dynamic_slice_in_dim(downs[core], start, depth, 0)
                total += dot32(block[:, core * depth : (core + 1) * depth], down)
            if step < 3:
                block = ring(block)
        home, away = total[: 2 * block_rows], total[2 * block_rows :]
        back = lax.ppermute(away.astype(jnp.bfloat16), "xl", SWAP)
        home = (home + back.astype(jnp.float32)).astype(jnp.bfloat16)
        home = home.reshape(2, EXPERTS, share, out_width).transpose(1, 0, 2, 3)
        home = home.reshape(EXPERTS, 2 * share * out_width // 128, 128)
        returned = lax.all_to_all(home, ("z", "xh"), 0, 0, tiled=True)
        returned = returned.reshape(EXPERTS * CAP // 2, out_width).astype(jnp.float32)
        slot = column % (CAP // 2) + half * (CAP // 2)
        combine = jnp.where(spread_rank == slot.astype(jnp.float32), spread_weight, 0.0)
        mixed += jnp.dot(
            combine, returned, precision=lax.Precision.HIGHEST, preferred_element_type=jnp.float32
        )
    return mixed.astype(jnp.bfloat16)


def solution(mesh):
    finer = Mesh(mesh.devices.reshape(16, 2, 2, 2, 4), EP_TP)
    placed = (
        P(EP, None),
        P(),
        P(EP, None),
        P(EP, None),
        P(None, EP_TP),
        P(None, EP_TP),
        P(EP, "y"),
    )
    return jax.shard_map(
        on_device, mesh=finer, in_specs=placed, out_specs=P(EP, "y"), check_vma=False
    )
```

```python
import jax
import jax.numpy as jnp
from jax import lax
from jax.sharding import Mesh
from jax.sharding import PartitionSpec as P


EPS = 1e-06
EP = ("z", "xh", "xl", "c")
EP_TP = ("z", "xh", "xl", "c", "y")
CAP = 12
SWAP = [(0, 1), (1, 0)]


def rms_rows(values, gain):
    widened = values.astype(jnp.float32)
    scale = lax.rsqrt(jnp.mean(widened * widened, axis=-1, keepdims=True) + EPS)
    return (widened * scale * gain).astype(jnp.bfloat16)


def shift(block, by=1):
    up = [(y, (y + by) % 4) for y in range(4)]
    down = [(4 + y, 4 + (y - by) % 4) for y in range(4)]
    return lax.ppermute(block, ("c", "y"), up + down)


def swap(block, axis):
    return lax.ppermute(block, axis, SWAP)


def dot32(a, b):
    return jnp.dot(a, b, preferred_element_type=jnp.float32)


def spread(per_expert, width, precision=None):
    count = per_expert.shape[1]
    expert = lax.broadcasted_iota(jnp.int32, (count, count * width), 1) // width
    own = lax.broadcasted_iota(jnp.int32, (count, count * width), 0)
    table = (expert == own).astype(per_expert.dtype)
    return jnp.dot(per_expert, table, precision=precision, preferred_element_type=jnp.float32)


def layer(tokens, norm_gain, expert_ids, gate_weights, w_gate, w_up, w_down):
    y = lax.axis_index("y")
    turn = 1 - 2 * lax.axis_index("c")
    rows = tokens.shape[0]
    width = tokens.shape[1]
    share = CAP // 4
    expert_count = lax.axis_size(("z", "xh"))
    block_rows = expert_count * share
    depth = w_gate.shape[1]
    out_width = w_down.shape[1]

    gate_x = swap(w_gate, "xl")
    up_x = swap(w_up, "xl")

    normed = rms_rows(tokens, norm_gain)
    experts = jnp.arange(expert_count, dtype=jnp.int32)[None, :]
    first = expert_ids[:, 0:1] == experts
    second = expert_ids[:, 1:2] == experts
    named = first | second
    weight = jnp.where(first, gate_weights[:, 0:1], 0.0) + jnp.where(
        second, gate_weights[:, 1:2], 0.0
    )
    earlier = (
        lax.broadcasted_iota(jnp.int32, (rows, rows), 0)
        > lax.broadcasted_iota(jnp.int32, (rows, rows), 1)
    ).astype(jnp.bfloat16)
    rank = dot32(earlier, named.astype(jnp.bfloat16))
    rank = jnp.where(named, rank, -1.0).astype(jnp.bfloat16)
    column = lax.broadcasted_iota(jnp.int32, (1, block_rows), 1)
    slot = share * y + column % share
    selector = (spread(rank, share) == slot.astype(jnp.float32)).astype(jnp.bfloat16)
    mine = lax.dot_general(
        selector, normed, (((0,), (0,)), ((), ())), preferred_element_type=jnp.float32
    ).astype(jnp.bfloat16)
    mine = mine.reshape(expert_count, share * width // 128, 128)
    arrived = lax.all_to_all(mine, ("z", "xh"), 0, 0, tiled=True)
    near = arrived.reshape(block_rows, width)

    cut = []
    for k in range(4):
        start = ((y + turn * k) & 3) * depth
        cut.append(lax.dynamic_slice_in_dim(w_down, start, depth, 0))
    for k in (1, 2, 3):
        cut[k] = shift(cut[k], k)
    down_o = (jnp.stack([cut[1], cut[3]]), jnp.stack([cut[2], cut[0]]))
    down_x = (swap(down_o[0], "xl"), swap(down_o[1], "xl"))
    gate_c = swap(w_gate, "c")
    up_c = swap(w_up, "c")
    down_c = (swap(down_o[0], "c"), swap(down_o[1], "c"))
    gate_d = swap(gate_x, "c")
    up_d = swap(up_x, "c")
    down_d = (swap(down_x[0], "c"), swap(down_x[1], "c"))

    halves = [near[: block_rows // 2], near[block_rows // 2 :]]
    gathered = list(halves)
    for _ in range(3):
        halves = [shift(halves[0]), shift(halves[1])]
        gathered += halves
    order = (0, 2, 1, 3)
    gathered = jnp.concatenate([gathered[2 * k + i] for k in order for i in range(2)], 0)

    gates = (w_gate, gate_c, gate_x, gate_d)
    uppers = (w_up, up_c, up_x, up_d)
    hidden = []
    for gate, up in zip(gates, uppers):
        gate_proj = dot32(gathered, gate)
        upper = dot32(gathered, up)
        hidden.append((jax.nn.silu(gate_proj) * upper).astype(jnp.bfloat16))

    def pick(pair, k):
        return pair[0][k // 2] if k % 2 else pair[1][0 if k else 1]

    half_rows = 2 * block_rows

    def partial(k):
        total = 0.0
        for matrix, pair, at in zip(
            hidden, (down_o, down_c, down_x, down_d), (k, (-k) % 4, k, (-k) % 4)
        ):
            total += dot32(matrix, pick(pair, at))
        return total

    total = partial(1)
    for step in (1, 2, 3):
        away = total.astype(jnp.bfloat16)
        back = [shift(away[:half_rows]), shift(away[half_rows:])]
        turned = [back[1][block_rows:], back[1][:block_rows], back[0]]
        total = partial((step + 1) % 4) + jnp.concatenate(turned, 0).astype(jnp.float32)
    home = total.astype(jnp.bfloat16)
    home = home.reshape(4, expert_count, share, out_width).transpose(1, 0, 2, 3)
    home = home.reshape(expert_count, CAP * out_width // 128, 128)
    returned = lax.all_to_all(home, ("z", "xh"), 0, 0, tiled=True)
    returned = returned.reshape(expert_count * CAP, out_width).astype(jnp.float32)
    column = lax.broadcasted_iota(jnp.int32, (1, expert_count * CAP), 1) % CAP
    place = column // share
    behind = 2 * (place % 2) + place // 2
    slot = share * ((y - turn * behind) & 3) + column % share
    chosen = spread(rank, CAP) == slot.astype(jnp.float32)
    combine = jnp.where(chosen, spread(weight, CAP, lax.Precision.HIGHEST), 0.0)
    mixed = jnp.dot(
        combine, returned, precision=lax.Precision.HIGHEST, preferred_element_type=jnp.float32
    )
    return mixed.astype(jnp.bfloat16)


def mapped(mesh):
    finer = Mesh(mesh.devices.reshape(-1, 2, 2, 2, 4), EP_TP)
    placed = (
        P(EP, None),
        P(),
        P(EP, None),
        P(EP, None),
        P(None, EP_TP),
        P(None, EP_TP),
        P(EP, "y"),
    )
    return jax.shard_map(layer, mesh=finer, in_specs=placed, out_specs=P(EP, "y"), check_vma=False)


def solution(mesh):
    return mapped(mesh)
```

```python
import jax
import jax.numpy as jnp
from jax import lax
from jax.sharding import Mesh
from jax.sharding import PartitionSpec as P


EPS = 1e-06
EP = ("z", "xh", "xl", "c")
EP_TP = ("z", "xh", "xl", "c", "y")
CAP = 12
SWAP = [(0, 1), (1, 0)]


def rms_rows(values, gain):
    widened = values.astype(jnp.float32)
    scale = lax.rsqrt(jnp.mean(widened * widened, axis=-1, keepdims=True) + EPS)
    return (widened * scale * gain).astype(jnp.bfloat16)


def shift(block, by=1):
    up = [(y, (y + by) % 4) for y in range(4)]
    down = [(4 + y, 4 + (y - by) % 4) for y in range(4)]
    return lax.ppermute(block, ("c", "y"), up + down)


def swap(block, axis):
    return lax.ppermute(block, axis, SWAP)


def dot32(a, b):
    return jnp.dot(a, b, preferred_element_type=jnp.float32)


def spread(per_expert, width, precision=None):
    count = per_expert.shape[1]
    expert = lax.broadcasted_iota(jnp.int32, (count, count * width), 1) // width
    own = lax.broadcasted_iota(jnp.int32, (count, count * width), 0)
    table = (expert == own).astype(per_expert.dtype)
    return jnp.dot(per_expert, table, precision=precision, preferred_element_type=jnp.float32)


def layer(tokens, norm_gain, expert_ids, gate_weights, w_gate, w_up, w_down):
    y = lax.axis_index("y")
    turn = 1 - 2 * lax.axis_index("c")
    rows = tokens.shape[0]
    width = tokens.shape[1]
    share = CAP // 4
    expert_count = lax.axis_size(("z", "xh"))
    block_rows = expert_count * share
    depth = w_gate.shape[1]
    out_width = w_down.shape[1]

    gate_x = swap(w_gate, "xl")
    up_x = swap(w_up, "xl")

    normed = rms_rows(tokens, norm_gain)
    experts = jnp.arange(expert_count, dtype=jnp.int32)[None, :]
    first = expert_ids[:, 0:1] == experts
    second = expert_ids[:, 1:2] == experts
    named = first | second
    weight = jnp.where(first, gate_weights[:, 0:1], 0.0) + jnp.where(
        second, gate_weights[:, 1:2], 0.0
    )
    earlier = (
        lax.broadcasted_iota(jnp.int32, (rows, rows), 0)
        > lax.broadcasted_iota(jnp.int32, (rows, rows), 1)
    ).astype(jnp.bfloat16)
    rank = dot32(earlier, named.astype(jnp.bfloat16))
    rank = jnp.where(named, rank, -1.0).astype(jnp.bfloat16)
    column = lax.broadcasted_iota(jnp.int32, (1, block_rows), 1)
    slot = share * y + column % share
    selector = (spread(rank, share) == slot.astype(jnp.float32)).astype(jnp.bfloat16)
    mine = lax.dot_general(
        selector, normed, (((0,), (0,)), ((), ())), preferred_element_type=jnp.float32
    ).astype(jnp.bfloat16)
    mine = mine.reshape(expert_count, share * width // 128, 128)
    arrived = lax.all_to_all(mine, ("z", "xh"), 0, 0, tiled=True)
    near = arrived.reshape(block_rows, width)

    cut = []
    for k in range(4):
        start = ((y + turn * k) & 3) * depth
        cut.append(lax.dynamic_slice_in_dim(w_down, start, depth, 0))
    for k in (1, 2, 3):
        cut[k] = shift(cut[k], k)
    down_o = (jnp.stack([cut[1], cut[3]]), jnp.stack([cut[2], cut[0]]))
    down_x = (swap(down_o[0], "xl"), swap(down_o[1], "xl"))
    gate_c = swap(w_gate, "c")
    up_c = swap(w_up, "c")
    down_c = (swap(down_o[0], "c"), swap(down_o[1], "c"))
    gate_d = swap(gate_x, "c")
    up_d = swap(up_x, "c")
    down_d = (swap(down_x[0], "c"), swap(down_x[1], "c"))

    blocks = [near]
    for _ in range(3):
        blocks.append(shift(blocks[-1]))

    hidden = []
    for gate, up in zip((w_gate, gate_c, gate_x, gate_d), (w_up, up_c, up_x, up_d)):
        parts = []
        for low in (0, 2):
            rows_now = jnp.concatenate(blocks[low : low + 2], 0)
            gate_proj = dot32(rows_now, gate)
            upper = dot32(rows_now, up)
            parts.append((jax.nn.silu(gate_proj) * upper).astype(jnp.bfloat16))
        hidden.append(jnp.concatenate(parts, 0))

    def pick(pair, k):
        return pair[0][k // 2] if k % 2 else pair[1][0 if k else 1]

    def partial(k):
        total = 0.0
        for matrix, pair, at in zip(
            hidden, (down_o, down_c, down_x, down_d), (k, (-k) % 4, k, (-k) % 4)
        ):
            total += dot32(matrix, pick(pair, at))
        return total

    total = partial(1)
    for step in (1, 2, 3):
        back = jnp.roll(shift(total.astype(jnp.bfloat16)), block_rows, 0)
        total = partial((step + 1) % 4) + back.astype(jnp.float32)
    home = total.astype(jnp.bfloat16)
    home = home.reshape(4, expert_count, share, out_width).transpose(1, 0, 2, 3)
    home = home.reshape(expert_count, CAP * out_width // 128, 128)
    returned = lax.all_to_all(home, ("z", "xh"), 0, 0, tiled=True)
    returned = returned.reshape(expert_count * CAP, out_width).astype(jnp.float32)
    column = lax.broadcasted_iota(jnp.int32, (1, expert_count * CAP), 1) % CAP
    slot = share * ((y - turn * (column // share)) & 3) + column % share
    chosen = spread(rank, CAP) == slot.astype(jnp.float32)
    combine = jnp.where(chosen, spread(weight, CAP, lax.Precision.HIGHEST), 0.0)
    mixed = jnp.dot(
        combine, returned, precision=lax.Precision.HIGHEST, preferred_element_type=jnp.float32
    )
    return mixed.astype(jnp.bfloat16)


def mapped(mesh):
    finer = Mesh(mesh.devices.reshape(-1, 2, 2, 2, 4), EP_TP)
    placed = (
        P(EP, None),
        P(),
        P(EP, None),
        P(EP, None),
        P(None, EP_TP),
        P(None, EP_TP),
        P(EP, "y"),
    )
    return jax.shard_map(
        layer, mesh=finer, in_specs=placed, out_specs=P(EP, "y"), check_vma=False
    )


def solution(mesh):
    return mapped(mesh)
```

```python
import jax
import jax.numpy as jnp
from jax import lax
from jax.experimental import pallas as pl
from jax.experimental.pallas import tpu as pltpu
from jax.sharding import Mesh
from jax.sharding import PartitionSpec as P


EPS = 1e-06
EP = ("z", "xh", "xl", "c")
EP_TP = ("z", "xh", "xl", "c", "y")
CAP = 12
SWAP = [(0, 1), (1, 0)]
TILE = 512


def rms_rows(values, gain):
    widened = values.astype(jnp.float32)
    scale = lax.rsqrt(jnp.mean(widened * widened, axis=-1, keepdims=True) + EPS)
    return (widened * scale * gain).astype(jnp.bfloat16)


def shift(block, by=1):
    up = [(y, (y + by) % 4) for y in range(4)]
    down = [(4 + y, 4 + (y - by) % 4) for y in range(4)]
    return lax.ppermute(block, ("c", "y"), up + down)


def swap(block, axis):
    return lax.ppermute(block, axis, SWAP)


def dot32(a, b):
    return jnp.dot(a, b, preferred_element_type=jnp.float32)


def spread(per_expert, width, precision=None):
    count = per_expert.shape[1]
    expert = lax.broadcasted_iota(jnp.int32, (count, count * width), 1) // width
    own = lax.broadcasted_iota(jnp.int32, (count, count * width), 0)
    table = (expert == own).astype(per_expert.dtype)
    return jnp.dot(per_expert, table, precision=precision, preferred_element_type=jnp.float32)


def hidden_kernel(rows_ref, gate_ref, up_ref, out_ref, gate_sum, up_sum):
    step = pl.program_id(0)

    @pl.when(step == 0)
    def _():
        gate_sum[...] = jnp.zeros_like(gate_sum)
        up_sum[...] = jnp.zeros_like(up_sum)

    tile = gate_ref.shape[0]
    rows = rows_ref[:, pl.ds(pl.multiple_of(step * tile, tile), tile)]
    gate_sum[...] += dot32(rows, gate_ref[...])
    up_sum[...] += dot32(rows, up_ref[...])

    @pl.when(step == pl.num_programs(0) - 1)
    def _():
        out_ref[...] = (jax.nn.silu(gate_sum[...]) * up_sum[...]).astype(out_ref.dtype)


def hidden_of(rows, weights):
    count, width = rows.shape
    depth = weights.shape[1]
    tile = min(TILE, width)
    steps = width // tile
    return pl.pallas_call(
        hidden_kernel,
        grid=(steps,),
        in_specs=[
            pl.BlockSpec(memory_space=pltpu.VMEM),
            pl.BlockSpec((tile, depth), lambda k: (k, 0)),
            pl.BlockSpec((tile, depth), lambda k: (steps + k, 0)),
        ],
        out_specs=pl.BlockSpec(memory_space=pltpu.VMEM),
        out_shape=jax.ShapeDtypeStruct((count, depth), jnp.bfloat16),
        scratch_shapes=[pltpu.VMEM((count, depth), jnp.float32)] * 2,
        cost_estimate=pl.CostEstimate(
            flops=4 * count * width * depth,
            bytes_accessed=2 * (count * width + 2 * width * depth + count * depth),
            transcendentals=count * depth,
        ),
        compiler_params=pltpu.CompilerParams(dimension_semantics=("arbitrary",)),
        name="hidden",
    )(rows, weights, weights)


def layer(tokens, norm_gain, expert_ids, gate_weights, w_gate, w_up, w_down):
    y = lax.axis_index("y")
    turn = 1 - 2 * lax.axis_index("c")
    rows = tokens.shape[0]
    width = tokens.shape[1]
    share = CAP // 4
    expert_count = lax.axis_size(("z", "xh"))
    block_rows = expert_count * share
    depth = w_gate.shape[1]
    out_width = w_down.shape[1]

    weights_o = jnp.concatenate([w_gate, w_up], 0)
    weights_x = swap(weights_o, "xl")
    down_x = swap(w_down, "xl")
    weights_c = swap(weights_o, "c")
    down_c = swap(w_down, "c")
    weights_d = swap(weights_x, "c")
    down_d = swap(down_x, "c")

    normed = rms_rows(tokens, norm_gain)
    experts = jnp.arange(expert_count, dtype=jnp.int32)[None, :]
    first = expert_ids[:, 0:1] == experts
    second = expert_ids[:, 1:2] == experts
    named = first | second
    weight = jnp.where(first, gate_weights[:, 0:1], 0.0) + jnp.where(
        second, gate_weights[:, 1:2], 0.0
    )
    earlier = (
        lax.broadcasted_iota(jnp.int32, (rows, rows), 0)
        > lax.broadcasted_iota(jnp.int32, (rows, rows), 1)
    ).astype(jnp.bfloat16)
    rank = dot32(earlier, named.astype(jnp.bfloat16))
    rank = jnp.where(named, rank, -1.0).astype(jnp.bfloat16)
    column = lax.broadcasted_iota(jnp.int32, (1, block_rows), 1)
    slot = share * y + column % share
    selector = (spread(rank, share) == slot.astype(jnp.float32)).astype(jnp.bfloat16)
    mine = lax.dot_general(
        selector, normed, (((0,), (0,)), ((), ())), preferred_element_type=jnp.float32
    ).astype(jnp.bfloat16)
    mine = mine.reshape(expert_count, share * width // 128, 128)
    arrived = lax.all_to_all(mine, ("z", "xh"), 0, 0, tiled=True)
    near = arrived.reshape(block_rows, width)

    blocks = [near]
    for _ in range(3):
        blocks.append(shift(blocks[-1]))

    gathered = jnp.concatenate(blocks, 0)

    near_pair = (hidden_of(gathered, weights_o), hidden_of(gathered, weights_c))
    far_pair = (hidden_of(gathered, weights_x), hidden_of(gathered, weights_d))
    near_steps = [jnp.concatenate(near_pair, 1)]
    far_steps = [jnp.concatenate(far_pair, 1)]
    for _ in range(3):
        near_steps.append(shift(near_steps[-1]))
        far_steps.append(shift(far_steps[-1]))
    for step in (0, 1):
        far_steps[step], _ = lax.optimization_barrier((far_steps[step], near_steps[2]))

    def down_of(steps, side, matrix):
        total = 0.0
        for step in range(4):
            start = ((y - turn * step) & 3) * depth
            turned = jnp.roll(steps[step], step * block_rows, 0)
            down = lax.dynamic_slice_in_dim(matrix, start, depth, 0)
            total += dot32(turned[:, side * depth : (side + 1) * depth], down)
        return total

    total = down_of(near_steps, 0, w_down) + down_of(near_steps, 1, down_c)
    total += down_of(far_steps, 0, down_x) + down_of(far_steps, 1, down_d)
    home = total.astype(jnp.bfloat16)
    home = home.reshape(4, expert_count, share, out_width).transpose(1, 0, 2, 3)
    home = home.reshape(expert_count, CAP * out_width // 128, 128)
    returned = lax.all_to_all(home, ("z", "xh"), 0, 0, tiled=True)
    returned = returned.reshape(expert_count * CAP, out_width).astype(jnp.float32)
    column = lax.broadcasted_iota(jnp.int32, (1, expert_count * CAP), 1) % CAP
    slot = share * ((y - turn * (column // share)) & 3) + column % share
    chosen = spread(rank, CAP) == slot.astype(jnp.float32)
    combine = jnp.where(chosen, spread(weight, CAP, lax.Precision.HIGHEST), 0.0)
    mixed = jnp.dot(
        combine, returned, precision=lax.Precision.HIGHEST, preferred_element_type=jnp.float32
    )
    return mixed.astype(jnp.bfloat16)


def mapped(mesh):
    finer = Mesh(mesh.devices.reshape(-1, 2, 2, 2, 4), EP_TP)
    placed = (
        P(EP, None),
        P(),
        P(EP, None),
        P(EP, None),
        P(None, EP_TP),
        P(None, EP_TP),
        P(EP, "y"),
    )
    return jax.shard_map(
        layer, mesh=finer, in_specs=placed, out_specs=P(EP, "y"), check_vma=False
    )


def solution(mesh):
    return mapped(mesh)
```

```python
import functools

import jax
import jax.numpy as jnp
from jax import lax
from jax.experimental import pallas as pl
from jax.experimental.pallas import tpu as pltpu
from jax.sharding import Mesh
from jax.sharding import PartitionSpec as P


EPS = 1e-06
EP = ("z", "xh", "xl", "c")
EP_TP = ("z", "xh", "xl", "c", "y")
CAP = 12
SWAP = [(0, 1), (1, 0)]


def rms_rows(values, gain):
    widened = values.astype(jnp.float32)
    scale = lax.rsqrt(jnp.mean(widened * widened, axis=-1, keepdims=True) + EPS)
    return (widened * scale * gain).astype(jnp.bfloat16)


def shift(block, by):
    return lax.ppermute(block, "y", [(y, (y + by) % 4) for y in range(4)])


def swap(block, axis):
    return lax.ppermute(block, axis, SWAP)


def dot32(a, b):
    return jnp.dot(a, b, preferred_element_type=jnp.float32)


def spread(per_expert, width, precision=None):
    count = per_expert.shape[1]
    expert = lax.broadcasted_iota(jnp.int32, (count, count * width), 1) // width
    own = lax.broadcasted_iota(jnp.int32, (count, count * width), 0)
    table = (expert == own).astype(per_expert.dtype)
    return jnp.dot(per_expert, table, precision=precision, preferred_element_type=jnp.float32)


def expert_kernel(*refs):
    rows_ref, gates, uppers, downs = refs[0], refs[1:5], refs[5:9], refs[9:13]
    hidden_ref, part_ref, wide, tall, sems = refs[13:]
    depth = wide.shape[2]
    copies = []
    for i in range(4):
        copies.append(pltpu.make_async_copy(gates[i], wide.at[2 * i], sems.at[3 * i]))
        copies.append(pltpu.make_async_copy(uppers[i], wide.at[2 * i + 1], sems.at[3 * i + 1]))
        copies.append(pltpu.make_async_copy(downs[i].at[2], tall.at[i], sems.at[3 * i + 2]))
    for copy in copies:
        copy.start()
    total = jnp.zeros(part_ref.shape, jnp.float32)
    for i in range(4):
        copies[3 * i].wait()
        gate_proj = dot32(rows_ref[...], wide[2 * i])
        copies[3 * i + 1].wait()
        upper = dot32(rows_ref[...], wide[2 * i + 1])
        piece = (jax.nn.silu(gate_proj) * upper).astype(jnp.bfloat16)
        hidden_ref[:, i * depth : (i + 1) * depth] = piece
        copies[3 * i + 2].wait()
        total += dot32(piece, tall[i])
    part_ref[...] = total.astype(part_ref.dtype)


def run_experts(rows_in, gates, uppers, downs):
    count, width = rows_in.shape
    depth = gates[0].shape[1]
    _, _, out_width = downs[0].shape
    return pl.pallas_call(
        expert_kernel,
        in_specs=[pl.BlockSpec(memory_space=pltpu.VMEM)]
        + [pl.BlockSpec(memory_space=pl.ANY)] * 12,
        out_specs=[pl.BlockSpec(memory_space=pltpu.VMEM)] * 2,
        out_shape=[
            jax.ShapeDtypeStruct((count, 4 * depth), jnp.bfloat16),
            jax.ShapeDtypeStruct((count, out_width), jnp.bfloat16),
        ],
        scratch_shapes=[
            pltpu.VMEM((8, width, depth), jnp.bfloat16),
            pltpu.VMEM((4, depth, out_width), jnp.bfloat16),
            pltpu.SemaphoreType.DMA((12,)),
        ],
        cost_estimate=pl.CostEstimate(
            flops=16 * count * width * depth,
            bytes_accessed=16 * width * depth,
            transcendentals=4 * count * depth,
        ),
        compiler_params=pltpu.CompilerParams(vmem_limit_bytes=40 << 20),
        name="experts",
    )(rows_in, *gates, *uppers, *downs)


def down_kernel(picks, hidden_ref, *refs):
    downs, outs, (tall, sems) = refs[:4], refs[4 : 4 + len(picks)], refs[4 + len(picks) :]
    depth = tall.shape[1]
    copies = [
        pltpu.make_async_copy(downs[i].at[k], tall.at[4 * n + i], sems.at[4 * n + i])
        for n, k in enumerate(picks)
        for i in range(4)
    ]
    for copy in copies:
        copy.start()
    for n, out in enumerate(outs):
        total = jnp.zeros(out.shape, jnp.float32)
        for i in range(4):
            copies[4 * n + i].wait()
            total += dot32(hidden_ref[:, i * depth : (i + 1) * depth], tall[4 * n + i])
        out[...] = total


def run_down(hidden, downs, picks):
    count = hidden.shape[0]
    _, depth, out_width = downs[0].shape
    return pl.pallas_call(
        functools.partial(down_kernel, picks),
        in_specs=[pl.BlockSpec(memory_space=pltpu.VMEM)] + [pl.BlockSpec(memory_space=pl.ANY)] * 4,
        out_specs=[pl.BlockSpec(memory_space=pltpu.VMEM)] * len(picks),
        out_shape=[jax.ShapeDtypeStruct((count, out_width), jnp.float32)] * len(picks),
        scratch_shapes=[
            pltpu.VMEM((4 * len(picks), depth, out_width), jnp.bfloat16),
            pltpu.SemaphoreType.DMA((4 * len(picks),)),
        ],
        cost_estimate=pl.CostEstimate(
            flops=8 * len(picks) * count * depth * out_width,
            bytes_accessed=8 * len(picks) * depth * out_width,
            transcendentals=0,
        ),
        compiler_params=pltpu.CompilerParams(vmem_limit_bytes=40 << 20),
        name="down",
    )(hidden, *downs)


def layer(tokens, norm_gain, expert_ids, gate_weights, w_gate, w_up, w_down):
    y = lax.axis_index("y")
    rows = tokens.shape[0]
    width = tokens.shape[1]
    share = CAP // 4
    expert_count = lax.axis_size(("z", "xh"))
    block_rows = expert_count * share
    depth = w_gate.shape[1]
    out_width = w_down.shape[1]

    gate_x = swap(w_gate, "xl")
    up_x = swap(w_up, "xl")

    normed = rms_rows(tokens, norm_gain)
    experts = jnp.arange(expert_count, dtype=jnp.int32)[None, :]
    first = expert_ids[:, 0:1] == experts
    second = expert_ids[:, 1:2] == experts
    named = first | second
    weight = jnp.where(first, gate_weights[:, 0:1], 0.0) + jnp.where(
        second, gate_weights[:, 1:2], 0.0
    )
    earlier = (
        lax.broadcasted_iota(jnp.int32, (rows, rows), 0)
        > lax.broadcasted_iota(jnp.int32, (rows, rows), 1)
    ).astype(jnp.bfloat16)
    rank = dot32(earlier, named.astype(jnp.bfloat16))
    rank = jnp.where(named, rank, -1.0).astype(jnp.bfloat16)
    column = lax.broadcasted_iota(jnp.int32, (1, block_rows), 1)
    slot = share * y + column % share
    selector = (spread(rank, share) == slot.astype(jnp.float32)).astype(jnp.bfloat16)
    mine = lax.dot_general(
        selector, normed, (((0,), (0,)), ((), ())), preferred_element_type=jnp.float32
    ).astype(jnp.bfloat16)
    mine = mine.reshape(expert_count, share * width // 128, 128)
    arrived = lax.all_to_all(mine, ("z", "xh"), 0, 0, tiled=True)
    near = arrived.reshape(block_rows, width)

    cut = []
    for k in range(4):
        start = ((y - k) & 3) * depth
        cut.append(lax.dynamic_slice_in_dim(w_down, start, depth, 0))
    for k in (1, 2, 3):
        cut[k] = shift(cut[k], -k)
    down_o = jnp.stack(cut)
    down_x = swap(down_o, "xl")
    gate_c = swap(w_gate, "c")
    up_c = swap(w_up, "c")
    down_c = swap(down_o, "c")
    gate_d = swap(gate_x, "c")
    up_d = swap(up_x, "c")
    down_d = swap(down_x, "c")

    half = block_rows // 2
    below = shift(near, 1)
    above = shift(near, -1)
    gathered = jnp.zeros((4, block_rows, width), jnp.bfloat16)
    for block, ahead in ((near, 0), (below, 3), (above, 1)):
        gathered = lax.dynamic_update_slice(gathered, block[None], ((y + ahead) & 3, 0, 0))
    for block, low in ((shift(below[:half], 1), 0), (shift(above[half:], -1), half)):
        gathered = lax.dynamic_update_slice(gathered, block[None], ((y + 2) & 3, low, 0))
    gathered = gathered.reshape(4 * block_rows, width)

    gates, uppers = (w_gate, gate_c, gate_x, gate_d), (w_up, up_c, up_x, up_d)
    downs = (down_o, down_c, down_x, down_d)
    hidden, away = run_experts(gathered, gates, uppers, downs)
    middle = 2 * block_rows
    first = shift(away[:middle], 1)
    second = shift(away[middle:], -1)
    upward, downward = run_down(hidden, downs, (1, 3))
    upward = jnp.concatenate([upward[:middle] + first.astype(jnp.float32), upward[middle:]], 0)
    downward = jnp.concatenate(
        [downward[:middle], downward[middle:] + second.astype(jnp.float32)], 0
    )
    first = shift(upward.astype(jnp.bfloat16), 1)
    second = shift(downward.astype(jnp.bfloat16), -1)
    (total,) = run_down(hidden, downs, (0,))
    total = total + first.astype(jnp.float32) + second.astype(jnp.float32)
    home = total.astype(jnp.bfloat16)
    home = home.reshape(4, expert_count, share, out_width).transpose(1, 0, 2, 3)
    home = home.reshape(expert_count, CAP * out_width // 128, 128)
    returned = lax.all_to_all(home, ("z", "xh"), 0, 0, tiled=True)
    returned = returned.reshape(expert_count * CAP, out_width).astype(jnp.float32)
    column = lax.broadcasted_iota(jnp.int32, (1, expert_count * CAP), 1) % CAP
    chosen = spread(rank, CAP) == column.astype(jnp.float32)
    combine = jnp.where(chosen, spread(weight, CAP, lax.Precision.HIGHEST), 0.0)
    mixed = jnp.dot(
        combine, returned, precision=lax.Precision.HIGHEST, preferred_element_type=jnp.float32
    )
    return mixed.astype(jnp.bfloat16)


def mapped(mesh):
    finer = Mesh(mesh.devices.reshape(-1, 2, 2, 2, 4), EP_TP)
    placed = (
        P(EP, None),
        P(),
        P(EP, None),
        P(EP, None),
        P(None, EP_TP),
        P(None, EP_TP),
        P(EP, "y"),
    )
    return jax.shard_map(layer, mesh=finer, in_specs=placed, out_specs=P(EP, "y"), check_vma=False)


def solution(mesh):
    return mapped(mesh)
```

```python
import functools

import jax
import jax.numpy as jnp
from jax import lax
from jax.experimental import pallas as pl
from jax.experimental.pallas import tpu as pltpu
from jax.sharding import Mesh
from jax.sharding import PartitionSpec as P


EPS = 1e-06
EP = ("z", "xh", "xl", "c")
EP_TP = ("z", "xh", "xl", "c", "y")
CAP = 12
SWAP = [(0, 1), (1, 0)]


def rms_rows(values, gain):
    widened = values.astype(jnp.float32)
    scale = lax.rsqrt(jnp.mean(widened * widened, axis=-1, keepdims=True) + EPS)
    return (widened * scale * gain).astype(jnp.bfloat16)


def shift(block, by):
    return lax.ppermute(block, "y", [(y, (y + by) % 4) for y in range(4)])


def turn(block):
    up = [(y, (y + 1) % 4) for y in range(4)]
    down = [(4 + y, 4 + (y - 1) % 4) for y in range(4)]
    return lax.ppermute(block, ("c", "y"), up + down)


def swap(block, axis):
    return lax.ppermute(block, axis, SWAP)


def dot32(a, b):
    return jnp.dot(a, b, preferred_element_type=jnp.float32)


def spread(per_expert, width, precision=None):
    count = per_expert.shape[1]
    expert = lax.broadcasted_iota(jnp.int32, (count, count * width), 1) // width
    own = lax.broadcasted_iota(jnp.int32, (count, count * width), 0)
    table = (expert == own).astype(per_expert.dtype)
    return jnp.dot(per_expert, table, precision=precision, preferred_element_type=jnp.float32)


def expert_kernel(at_ref, *refs):
    blocks, gates, uppers, downs = refs[0:4], refs[4:8], refs[8:12], refs[12:16]
    hidden_ref, part_ref, rows, wide, tall, sems, row_sems = refs[16:]
    depth = wide.shape[2]
    count = blocks[0].shape[0]
    moves, copies = [], []
    for i in range(4):
        place = pl.ds(pl.multiple_of(((at_ref[0] + i) & 3) * count, 16), count)
        moves.append(pltpu.make_async_copy(blocks[i], rows.at[place], row_sems.at[i]))
    for i in range(4):
        copies.append(pltpu.make_async_copy(gates[i], wide.at[2 * i], sems.at[3 * i]))
        copies.append(pltpu.make_async_copy(uppers[i], wide.at[2 * i + 1], sems.at[3 * i + 1]))
        copies.append(pltpu.make_async_copy(downs[i].at[2], tall.at[i], sems.at[3 * i + 2]))
    for copy in moves + copies:
        copy.start()
    for move in moves:
        move.wait()
    total = jnp.zeros(part_ref.shape, jnp.float32)
    for i in range(4):
        copies[3 * i].wait()
        gate_proj = dot32(rows[...], wide[2 * i])
        copies[3 * i + 1].wait()
        upper = dot32(rows[...], wide[2 * i + 1])
        piece = (jax.nn.silu(gate_proj) * upper).astype(jnp.bfloat16)
        hidden_ref[:, i * depth : (i + 1) * depth] = piece
        copies[3 * i + 2].wait()
        total += dot32(piece, tall[i])
    part_ref[...] = total.astype(part_ref.dtype)


def run_experts(at, blocks, gates, uppers, downs):
    count, width = 4 * blocks[0].shape[0], blocks[0].shape[1]
    depth = gates[0].shape[1]
    _, _, out_width = downs[0].shape
    return pl.pallas_call(
        expert_kernel,
        in_specs=[pl.BlockSpec(memory_space=pltpu.SMEM)]
        + [pl.BlockSpec(memory_space=pl.ANY)] * 16,
        out_specs=[pl.BlockSpec(memory_space=pltpu.VMEM)] * 2,
        out_shape=[
            jax.ShapeDtypeStruct((count, 4 * depth), jnp.bfloat16),
            jax.ShapeDtypeStruct((count, out_width), jnp.bfloat16),
        ],
        scratch_shapes=[
            pltpu.VMEM((count, width), jnp.bfloat16),
            pltpu.VMEM((8, width, depth), jnp.bfloat16),
            pltpu.VMEM((4, depth, out_width), jnp.bfloat16),
            pltpu.SemaphoreType.DMA((12,)),
            pltpu.SemaphoreType.DMA((4,)),
        ],
        cost_estimate=pl.CostEstimate(
            flops=16 * count * width * depth,
            bytes_accessed=16 * width * depth,
            transcendentals=4 * count * depth,
        ),
        compiler_params=pltpu.CompilerParams(vmem_limit_bytes=20 << 20),
        name="experts",
    )(at, *blocks, *gates, *uppers, *downs)


def down_kernel(picks, hidden_ref, *refs):
    downs, outs, (tall, sems) = refs[:4], refs[4 : 4 + len(picks)], refs[4 + len(picks) :]
    depth = tall.shape[1]
    copies = [
        pltpu.make_async_copy(downs[i].at[k], tall.at[4 * n + i], sems.at[4 * n + i])
        for n, k in enumerate(picks)
        for i in range(4)
    ]
    for copy in copies:
        copy.start()
    for n, out in enumerate(outs):
        total = jnp.zeros(out.shape, jnp.float32)
        for i in range(4):
            copies[4 * n + i].wait()
            total += dot32(hidden_ref[:, i * depth : (i + 1) * depth], tall[4 * n + i])
        out[...] = total


def run_down(hidden, downs, picks):
    count = hidden.shape[0]
    _, depth, out_width = downs[0].shape
    return pl.pallas_call(
        functools.partial(down_kernel, picks),
        in_specs=[pl.BlockSpec(memory_space=pltpu.VMEM)] + [pl.BlockSpec(memory_space=pl.ANY)] * 4,
        out_specs=[pl.BlockSpec(memory_space=pltpu.VMEM)] * len(picks),
        out_shape=[jax.ShapeDtypeStruct((count, out_width), jnp.float32)] * len(picks),
        scratch_shapes=[
            pltpu.VMEM((4 * len(picks), depth, out_width), jnp.bfloat16),
            pltpu.SemaphoreType.DMA((4 * len(picks),)),
        ],
        cost_estimate=pl.CostEstimate(
            flops=8 * len(picks) * count * depth * out_width,
            bytes_accessed=8 * len(picks) * depth * out_width,
            transcendentals=0,
        ),
        compiler_params=pltpu.CompilerParams(vmem_limit_bytes=12 << 20),
        name="down",
    )(hidden, *downs)


def layer(tokens, norm_gain, expert_ids, gate_weights, w_gate, w_up, w_down):
    y = lax.axis_index("y")
    rows = tokens.shape[0]
    width = tokens.shape[1]
    share = CAP // 4
    expert_count = lax.axis_size(("z", "xh"))
    block_rows = expert_count * share
    depth = w_gate.shape[1]
    out_width = w_down.shape[1]

    gate_x = swap(w_gate, "xl")
    up_x = swap(w_up, "xl")

    normed = rms_rows(tokens, norm_gain)
    experts = jnp.arange(expert_count, dtype=jnp.int32)[None, :]
    first = expert_ids[:, 0:1] == experts
    second = expert_ids[:, 1:2] == experts
    named = first | second
    weight = jnp.where(first, gate_weights[:, 0:1], 0.0) + jnp.where(
        second, gate_weights[:, 1:2], 0.0
    )
    earlier = (
        lax.broadcasted_iota(jnp.int32, (rows, rows), 0)
        > lax.broadcasted_iota(jnp.int32, (rows, rows), 1)
    ).astype(jnp.bfloat16)
    rank = dot32(earlier, named.astype(jnp.bfloat16))
    rank = jnp.where(named, rank, -1.0).astype(jnp.bfloat16)
    column = lax.broadcasted_iota(jnp.int32, (1, block_rows), 1)
    slot = share * y + column % share
    selector = (spread(rank, share) == slot.astype(jnp.float32)).astype(jnp.bfloat16)
    mine = lax.dot_general(
        selector, normed, (((0,), (0,)), ((), ())), preferred_element_type=jnp.float32
    ).astype(jnp.bfloat16)
    mine = mine.reshape(expert_count, share * width // 128, 128)
    arrived = lax.all_to_all(mine, ("z", "xh"), 0, 0, tiled=True)
    near = arrived.reshape(block_rows, width)

    cut = []
    for k in range(4):
        start = ((y - k) & 3) * depth
        cut.append(lax.dynamic_slice_in_dim(w_down, start, depth, 0))
    for k in (1, 2, 3):
        cut[k] = shift(cut[k], -k)
    down_o = jnp.stack(cut)
    down_x = swap(down_o, "xl")
    gate_c = swap(w_gate, "c")
    up_c = swap(w_up, "c")
    down_c = swap(down_o, "c")
    gate_d = swap(gate_x, "c")
    up_d = swap(up_x, "c")
    down_d = swap(down_x, "c")

    lower_core = lax.axis_index("c") == 0
    below = shift(near, 1)
    above = shift(near, -1)
    across = turn(jnp.where(lower_core, below, above))
    blocks = (near, above, across, below)
    gates, uppers = (w_gate, gate_c, gate_x, gate_d), (w_up, up_c, up_x, up_d)
    downs = (down_o, down_c, down_x, down_d)
    hidden, away = run_experts(y[None].astype(jnp.int32), blocks, gates, uppers, downs)
    middle = turn(away).astype(jnp.float32)
    upward, downward = run_down(hidden, downs, (1, 3))
    upward += jnp.where(lower_core, middle, 0.0)
    downward += jnp.where(lower_core, 0.0, middle)
    first = shift(upward.astype(jnp.bfloat16), 1)
    second = shift(downward.astype(jnp.bfloat16), -1)
    (total,) = run_down(hidden, downs, (0,))
    total = total + first.astype(jnp.float32) + second.astype(jnp.float32)
    home = total.astype(jnp.bfloat16)
    home = home.reshape(4, expert_count, share, out_width).transpose(1, 0, 2, 3)
    home = home.reshape(expert_count, CAP * out_width // 128, 128)
    returned = lax.all_to_all(home, ("z", "xh"), 0, 0, tiled=True)
    returned = returned.reshape(expert_count * CAP, out_width).astype(jnp.float32)
    column = lax.broadcasted_iota(jnp.int32, (1, expert_count * CAP), 1) % CAP
    chosen = spread(rank, CAP) == column.astype(jnp.float32)
    combine = jnp.where(chosen, spread(weight, CAP, lax.Precision.HIGHEST), 0.0)
    mixed = jnp.dot(
        combine, returned, precision=lax.Precision.HIGHEST, preferred_element_type=jnp.float32
    )
    return mixed.astype(jnp.bfloat16)


def mapped(mesh):
    finer = Mesh(mesh.devices.reshape(-1, 2, 2, 2, 4), EP_TP)
    placed = (
        P(EP, None),
        P(),
        P(EP, None),
        P(EP, None),
        P(None, EP_TP),
        P(None, EP_TP),
        P(EP, "y"),
    )
    return jax.shard_map(layer, mesh=finer, in_specs=placed, out_specs=P(EP, "y"), check_vma=False)


def solution(mesh):
    return mapped(mesh)
```

```python
import functools

import jax
import jax.numpy as jnp
from jax import lax
from jax.experimental import pallas as pl
from jax.experimental.pallas import tpu as pltpu
from jax.sharding import Mesh
from jax.sharding import PartitionSpec as P


EPS = 1e-06
EP = ("z", "xh", "xl", "c")
EP_TP = ("z", "xh", "xl", "c", "y")
CAP = 12
SWAP = [(0, 1), (1, 0)]


def rms_rows(values, gain):
    widened = values.astype(jnp.float32)
    scale = lax.rsqrt(jnp.mean(widened * widened, axis=-1, keepdims=True) + EPS)
    return (widened * scale * gain).astype(jnp.bfloat16)


def shift(block, by):
    return lax.ppermute(block, "y", [(y, (y + by) % 4) for y in range(4)])


def turn(block):
    up = [(y, (y + 1) % 4) for y in range(4)]
    down = [(4 + y, 4 + (y - 1) % 4) for y in range(4)]
    return lax.ppermute(block, ("c", "y"), up + down)


def swap(block, axis):
    return lax.ppermute(block, axis, SWAP)


def dot32(a, b):
    return jnp.dot(a, b, preferred_element_type=jnp.float32)


def spread(per_expert, width, precision=None):
    count = per_expert.shape[1]
    expert = lax.broadcasted_iota(jnp.int32, (count, count * width), 1) // width
    own = lax.broadcasted_iota(jnp.int32, (count, count * width), 0)
    table = (expert == own).astype(per_expert.dtype)
    return jnp.dot(per_expert, table, precision=precision, preferred_element_type=jnp.float32)


def expert_kernel(at_ref, *refs):
    blocks, gates, uppers, downs = refs[0:4], refs[4:8], refs[8:12], refs[12:16]
    hidden_ref, part_ref, rows, wide, tall, sems, row_sems = refs[16:]
    depth = wide.shape[2]
    count = blocks[0].shape[0]
    moves, copies = [], []
    for i in range(4):
        place = pl.ds(pl.multiple_of(((at_ref[0] + i) & 3) * count, 16), count)
        moves.append(pltpu.make_async_copy(blocks[i], rows.at[place], row_sems.at[i]))
    for i in range(4):
        copies.append(pltpu.make_async_copy(gates[i], wide.at[2 * i], sems.at[3 * i]))
        copies.append(pltpu.make_async_copy(uppers[i], wide.at[2 * i + 1], sems.at[3 * i + 1]))
        copies.append(pltpu.make_async_copy(downs[i], tall.at[i], sems.at[3 * i + 2]))
    for copy in moves + copies:
        copy.start()
    for move in moves:
        move.wait()
    total = jnp.zeros(part_ref.shape, jnp.float32)
    for i in range(4):
        copies[3 * i].wait()
        gate_proj = dot32(rows[...], wide[2 * i])
        copies[3 * i + 1].wait()
        upper = dot32(rows[...], wide[2 * i + 1])
        piece = (jax.nn.silu(gate_proj) * upper).astype(jnp.bfloat16)
        hidden_ref[:, i * depth : (i + 1) * depth] = piece
        copies[3 * i + 2].wait()
        total += dot32(piece, tall[i])
    part_ref[...] = total.astype(part_ref.dtype)


def run_experts(at, blocks, gates, uppers, downs):
    count, width = 4 * blocks[0].shape[0], blocks[0].shape[1]
    depth = gates[0].shape[1]
    out_width = downs[0].shape[1]
    return pl.pallas_call(
        expert_kernel,
        in_specs=[pl.BlockSpec(memory_space=pltpu.SMEM)]
        + [pl.BlockSpec(memory_space=pl.ANY)] * 16,
        out_specs=[pl.BlockSpec(memory_space=pltpu.VMEM)] * 2,
        out_shape=[
            jax.ShapeDtypeStruct((count, 4 * depth), jnp.bfloat16),
            jax.ShapeDtypeStruct((count, out_width), jnp.bfloat16),
        ],
        scratch_shapes=[
            pltpu.VMEM((count, width), jnp.bfloat16),
            pltpu.VMEM((8, width, depth), jnp.bfloat16),
            pltpu.VMEM((4, depth, out_width), jnp.bfloat16),
            pltpu.SemaphoreType.DMA((12,)),
            pltpu.SemaphoreType.DMA((4,)),
        ],
        cost_estimate=pl.CostEstimate(
            flops=16 * count * width * depth,
            bytes_accessed=16 * width * depth,
            transcendentals=4 * count * depth,
        ),
        compiler_params=pltpu.CompilerParams(vmem_limit_bytes=20 << 20),
        name="experts",
    )(at, *blocks, *gates, *uppers, *downs)


def down_kernel(picks, hidden_ref, *refs):
    downs, outs, (tall, sems) = refs[:4], refs[4 : 4 + len(picks)], refs[4 + len(picks) :]
    depth = tall.shape[1]
    copies = [
        pltpu.make_async_copy(downs[i].at[k], tall.at[4 * n + i], sems.at[4 * n + i])
        for n, k in enumerate(picks)
        for i in range(4)
    ]
    for copy in copies:
        copy.start()
    for n, out in enumerate(outs):
        total = jnp.zeros(out.shape, jnp.float32)
        for i in range(4):
            copies[4 * n + i].wait()
            total += dot32(hidden_ref[:, i * depth : (i + 1) * depth], tall[4 * n + i])
        out[...] = total


def run_down(hidden, downs, picks):
    count = hidden.shape[0]
    _, depth, out_width = downs[0].shape
    return pl.pallas_call(
        functools.partial(down_kernel, picks),
        in_specs=[pl.BlockSpec(memory_space=pltpu.VMEM)] + [pl.BlockSpec(memory_space=pl.ANY)] * 4,
        out_specs=[pl.BlockSpec(memory_space=pltpu.VMEM)] * len(picks),
        out_shape=[jax.ShapeDtypeStruct((count, out_width), jnp.float32)] * len(picks),
        scratch_shapes=[
            pltpu.VMEM((4 * len(picks), depth, out_width), jnp.bfloat16),
            pltpu.SemaphoreType.DMA((4 * len(picks),)),
        ],
        cost_estimate=pl.CostEstimate(
            flops=8 * len(picks) * count * depth * out_width,
            bytes_accessed=8 * len(picks) * depth * out_width,
            transcendentals=0,
        ),
        compiler_params=pltpu.CompilerParams(vmem_limit_bytes=12 << 20),
        name="down",
    )(hidden, *downs)


def layer(tokens, norm_gain, expert_ids, gate_weights, w_gate, w_up, w_down):
    y = lax.axis_index("y")
    rows = tokens.shape[0]
    width = tokens.shape[1]
    share = CAP // 4
    expert_count = lax.axis_size(("z", "xh"))
    block_rows = expert_count * share
    depth = w_gate.shape[1]
    out_width = w_down.shape[1]

    gate_x = swap(w_gate, "xl")
    up_x = swap(w_up, "xl")

    normed = rms_rows(tokens, norm_gain)
    experts = jnp.arange(expert_count, dtype=jnp.int32)[None, :]
    first = expert_ids[:, 0:1] == experts
    second = expert_ids[:, 1:2] == experts
    named = first | second
    weight = jnp.where(first, gate_weights[:, 0:1], 0.0) + jnp.where(
        second, gate_weights[:, 1:2], 0.0
    )
    earlier = (
        lax.broadcasted_iota(jnp.int32, (rows, rows), 0)
        > lax.broadcasted_iota(jnp.int32, (rows, rows), 1)
    ).astype(jnp.bfloat16)
    rank = dot32(earlier, named.astype(jnp.bfloat16))
    rank = jnp.where(named, rank, -1.0).astype(jnp.bfloat16)
    column = lax.broadcasted_iota(jnp.int32, (1, block_rows), 1)
    slot = share * y + column % share
    selector = (spread(rank, share) == slot.astype(jnp.float32)).astype(jnp.bfloat16)
    mine = lax.dot_general(
        selector, normed, (((0,), (0,)), ((), ())), preferred_element_type=jnp.float32
    ).astype(jnp.bfloat16)
    mine = mine.reshape(expert_count, share * width // 128, 128)
    arrived = lax.all_to_all(mine, ("z", "xh"), 0, 0, tiled=True)
    near = arrived.reshape(block_rows, width)

    cut = []
    for k in range(4):
        start = ((y - k) & 3) * depth
        cut.append(lax.dynamic_slice_in_dim(w_down, start, depth, 0))
    for k in (2, 1, 3):
        cut[k] = shift(cut[k], -k)
    gate_c = swap(w_gate, "c")
    up_c = swap(w_up, "c")
    leads = [cut[2], swap(cut[2], "c"), swap(cut[2], "xl")]
    leads.append(swap(leads[2], "c"))
    rest = jnp.stack([cut[1], cut[3], cut[0]])
    rests = [rest, swap(rest, "c"), swap(rest, "xl")]
    rests.append(swap(rests[2], "c"))
    gate_d = swap(gate_x, "c")
    up_d = swap(up_x, "c")

    lower_core = lax.axis_index("c") == 0
    below = shift(near, 1)
    above = shift(near, -1)
    across = turn(jnp.where(lower_core, below, above))
    blocks = (near, above, across, below)
    gates, uppers = (w_gate, gate_c, gate_x, gate_d), (w_up, up_c, up_x, up_d)
    hidden, away = run_experts(y[None].astype(jnp.int32), blocks, gates, uppers, leads)
    middle = turn(away).astype(jnp.float32)
    upward, downward = run_down(hidden, rests, (0, 1))
    upward += jnp.where(lower_core, middle, 0.0)
    downward += jnp.where(lower_core, 0.0, middle)
    first = shift(upward.astype(jnp.bfloat16), 1)
    second = shift(downward.astype(jnp.bfloat16), -1)
    (total,) = run_down(hidden, rests, (2,))
    total = total + first.astype(jnp.float32) + second.astype(jnp.float32)
    home = total.astype(jnp.bfloat16)
    home = home.reshape(4, expert_count, share, out_width).transpose(1, 0, 2, 3)
    home = home.reshape(expert_count, CAP * out_width // 128, 128)
    returned = lax.all_to_all(home, ("z", "xh"), 0, 0, tiled=True)
    returned = returned.reshape(expert_count * CAP, out_width).astype(jnp.float32)
    column = lax.broadcasted_iota(jnp.int32, (1, expert_count * CAP), 1) % CAP
    chosen = spread(rank, CAP) == column.astype(jnp.float32)
    combine = jnp.where(chosen, spread(weight, CAP, lax.Precision.HIGHEST), 0.0)
    mixed = jnp.dot(
        combine, returned, precision=lax.Precision.HIGHEST, preferred_element_type=jnp.float32
    )
    return mixed.astype(jnp.bfloat16)


def mapped(mesh):
    finer = Mesh(mesh.devices.reshape(-1, 2, 2, 2, 4), EP_TP)
    placed = (
        P(EP, None),
        P(),
        P(EP, None),
        P(EP, None),
        P(None, EP_TP),
        P(None, EP_TP),
        P(EP, "y"),
    )
    return jax.shard_map(layer, mesh=finer, in_specs=placed, out_specs=P(EP, "y"), check_vma=False)


def solution(mesh):
    return mapped(mesh)
```

```python
import functools

import jax
import jax.numpy as jnp
from jax import lax
from jax.experimental import pallas as pl
from jax.experimental.pallas import tpu as pltpu
from jax.sharding import Mesh
from jax.sharding import PartitionSpec as P


EPS = 1e-06
EP = ("z", "xh", "xl", "c")
EP_TP = ("z", "xh", "xl", "c", "y")
CAP = 12
SWAP = [(0, 1), (1, 0)]


def rms_rows(values, gain):
    widened = values.astype(jnp.float32)
    scale = lax.rsqrt(jnp.mean(widened * widened, axis=-1, keepdims=True) + EPS)
    return (widened * scale * gain).astype(jnp.bfloat16)


def shift(block, by):
    return lax.ppermute(block, "y", [(y, (y + by) % 4) for y in range(4)])


def turn(block):
    up = [(y, (y + 1) % 4) for y in range(4)]
    down = [(4 + y, 4 + (y - 1) % 4) for y in range(4)]
    return lax.ppermute(block, ("c", "y"), up + down)


def swap(block, axis):
    return lax.ppermute(block, axis, SWAP)


def dot32(a, b):
    return jnp.dot(a, b, preferred_element_type=jnp.float32)


def spread(per_expert, width, precision=None):
    count = per_expert.shape[1]
    expert = lax.broadcasted_iota(jnp.int32, (count, count * width), 1) // width
    own = lax.broadcasted_iota(jnp.int32, (count, count * width), 0)
    table = (expert == own).astype(per_expert.dtype)
    return jnp.dot(per_expert, table, precision=precision, preferred_element_type=jnp.float32)


def expert_kernel(at_ref, *refs):
    blocks, gates, uppers, downs = refs[0:4], refs[4:8], refs[8:12], refs[12:16]
    hidden_ref, part_ref, rows, wide, tall, sems, row_sems = refs[16:]
    depth = wide.shape[2] // 2
    count = blocks[0].shape[0]
    moves, copies = [], []
    for i in range(4):
        place = pl.ds(pl.multiple_of(((at_ref[0] + i) & 3) * count, 16), count)
        moves.append(pltpu.make_async_copy(blocks[i], rows.at[place], row_sems.at[i]))
    for i in range(4):
        gate_at, up_at = wide.at[i, :, pl.ds(0, depth)], wide.at[i, :, pl.ds(depth, depth)]
        copies.append(pltpu.make_async_copy(gates[i], gate_at, sems.at[3 * i]))
        copies.append(pltpu.make_async_copy(uppers[i], up_at, sems.at[3 * i + 1]))
        copies.append(pltpu.make_async_copy(downs[i], tall.at[i], sems.at[3 * i + 2]))
    for copy in moves + copies:
        copy.start()
    for move in moves:
        move.wait()
    total = jnp.zeros(part_ref.shape, jnp.float32)
    for i in range(4):
        copies[3 * i].wait()
        copies[3 * i + 1].wait()
        both = dot32(rows[...], wide[i])
        piece = (jax.nn.silu(both[:, :depth]) * both[:, depth:]).astype(jnp.bfloat16)
        hidden_ref[:, i * depth : (i + 1) * depth] = piece
        copies[3 * i + 2].wait()
        total += dot32(piece, tall[i])
    part_ref[...] = total.astype(part_ref.dtype)


def run_experts(at, blocks, gates, uppers, downs):
    count, width = 4 * blocks[0].shape[0], blocks[0].shape[1]
    depth = gates[0].shape[1]
    out_width = downs[0].shape[1]
    return pl.pallas_call(
        expert_kernel,
        in_specs=[pl.BlockSpec(memory_space=pltpu.SMEM)]
        + [pl.BlockSpec(memory_space=pl.ANY)] * 16,
        out_specs=[pl.BlockSpec(memory_space=pltpu.VMEM)] * 2,
        out_shape=[
            jax.ShapeDtypeStruct((count, 4 * depth), jnp.bfloat16),
            jax.ShapeDtypeStruct((count, out_width), jnp.bfloat16),
        ],
        scratch_shapes=[
            pltpu.VMEM((count, width), jnp.bfloat16),
            pltpu.VMEM((4, width, 2 * depth), jnp.bfloat16),
            pltpu.VMEM((4, depth, out_width), jnp.bfloat16),
            pltpu.SemaphoreType.DMA((12,)),
            pltpu.SemaphoreType.DMA((4,)),
        ],
        cost_estimate=pl.CostEstimate(
            flops=16 * count * width * depth,
            bytes_accessed=16 * width * depth,
            transcendentals=4 * count * depth,
        ),
        compiler_params=pltpu.CompilerParams(vmem_limit_bytes=20 << 20),
        name="experts",
    )(at, *blocks, *gates, *uppers, *downs)


def down_kernel(picks, hidden_ref, *refs):
    downs, outs, (tall, sems) = refs[:4], refs[4 : 4 + len(picks)], refs[4 + len(picks) :]
    depth = tall.shape[1]
    copies = [
        pltpu.make_async_copy(downs[i].at[k], tall.at[4 * n + i], sems.at[4 * n + i])
        for n, k in enumerate(picks)
        for i in range(4)
    ]
    for copy in copies:
        copy.start()
    for n, out in enumerate(outs):
        total = jnp.zeros(out.shape, jnp.float32)
        for i in range(4):
            copies[4 * n + i].wait()
            total += dot32(hidden_ref[:, i * depth : (i + 1) * depth], tall[4 * n + i])
        out[...] = total


def run_down(hidden, downs, picks):
    count = hidden.shape[0]
    _, depth, out_width = downs[0].shape
    return pl.pallas_call(
        functools.partial(down_kernel, picks),
        in_specs=[pl.BlockSpec(memory_space=pltpu.VMEM)] + [pl.BlockSpec(memory_space=pl.ANY)] * 4,
        out_specs=[pl.BlockSpec(memory_space=pltpu.VMEM)] * len(picks),
        out_shape=[jax.ShapeDtypeStruct((count, out_width), jnp.float32)] * len(picks),
        scratch_shapes=[
            pltpu.VMEM((4 * len(picks), depth, out_width), jnp.bfloat16),
            pltpu.SemaphoreType.DMA((4 * len(picks),)),
        ],
        cost_estimate=pl.CostEstimate(
            flops=8 * len(picks) * count * depth * out_width,
            bytes_accessed=8 * len(picks) * depth * out_width,
            transcendentals=0,
        ),
        compiler_params=pltpu.CompilerParams(vmem_limit_bytes=12 << 20),
        name="down",
    )(hidden, *downs)


def layer(tokens, norm_gain, expert_ids, gate_weights, w_gate, w_up, w_down):
    y = lax.axis_index("y")
    rows = tokens.shape[0]
    width = tokens.shape[1]
    share = CAP // 4
    expert_count = lax.axis_size(("z", "xh"))
    block_rows = expert_count * share
    depth = w_gate.shape[1]
    out_width = w_down.shape[1]

    gate_x = swap(w_gate, "xl")
    up_x = swap(w_up, "xl")

    normed = rms_rows(tokens, norm_gain)
    experts = jnp.arange(expert_count, dtype=jnp.int32)[None, :]
    first = expert_ids[:, 0:1] == experts
    second = expert_ids[:, 1:2] == experts
    named = first | second
    weight = jnp.where(first, gate_weights[:, 0:1], 0.0) + jnp.where(
        second, gate_weights[:, 1:2], 0.0
    )
    earlier = (
        lax.broadcasted_iota(jnp.int32, (rows, rows), 0)
        > lax.broadcasted_iota(jnp.int32, (rows, rows), 1)
    ).astype(jnp.bfloat16)
    rank = dot32(earlier, named.astype(jnp.bfloat16))
    rank = jnp.where(named, rank, -1.0).astype(jnp.bfloat16)
    column = lax.broadcasted_iota(jnp.int32, (1, block_rows), 1)
    slot = share * y + column % share
    selector = (spread(rank, share) == slot.astype(jnp.float32)).astype(jnp.bfloat16)
    mine = lax.dot_general(
        selector, normed, (((0,), (0,)), ((), ())), preferred_element_type=jnp.float32
    ).astype(jnp.bfloat16)
    mine = mine.reshape(expert_count, share * width // 128, 128)
    arrived = lax.all_to_all(mine, ("z", "xh"), 0, 0, tiled=True)
    near = arrived.reshape(block_rows, width)

    cut = []
    for k in range(4):
        start = ((y - k) & 3) * depth
        cut.append(lax.dynamic_slice_in_dim(w_down, start, depth, 0))
    for k in (2, 1, 3):
        cut[k] = shift(cut[k], -k)
    gate_c = swap(w_gate, "c")
    up_c = swap(w_up, "c")
    leads = [cut[2], swap(cut[2], "c"), swap(cut[2], "xl")]
    leads.append(swap(leads[2], "c"))
    rest = jnp.stack([cut[1], cut[3], cut[0]])
    rests = [rest, swap(rest, "c"), swap(rest, "xl")]
    rests.append(swap(rests[2], "c"))
    gate_d = swap(gate_x, "c")
    up_d = swap(up_x, "c")

    lower_core = lax.axis_index("c") == 0
    below = shift(near, 1)
    above = shift(near, -1)
    across = turn(jnp.where(lower_core, below, above))
    blocks = (near, above, across, below)
    gates, uppers = (w_gate, gate_c, gate_x, gate_d), (w_up, up_c, up_x, up_d)
    hidden, away = run_experts(y[None].astype(jnp.int32), blocks, gates, uppers, leads)
    middle = turn(away).astype(jnp.float32)
    upward, downward = run_down(hidden, rests, (0, 1))
    upward += jnp.where(lower_core, middle, 0.0)
    downward += jnp.where(lower_core, 0.0, middle)
    first = shift(upward.astype(jnp.bfloat16), 1)
    second = shift(downward.astype(jnp.bfloat16), -1)
    (total,) = run_down(hidden, rests, (2,))
    total = total + first.astype(jnp.float32) + second.astype(jnp.float32)
    home = total.astype(jnp.bfloat16)
    home = home.reshape(4, expert_count, share, out_width).transpose(1, 0, 2, 3)
    home = home.reshape(expert_count, CAP * out_width // 128, 128)
    returned = lax.all_to_all(home, ("z", "xh"), 0, 0, tiled=True)
    returned = returned.reshape(expert_count * CAP, out_width).astype(jnp.float32)
    column = lax.broadcasted_iota(jnp.int32, (1, expert_count * CAP), 1) % CAP
    chosen = spread(rank, CAP) == column.astype(jnp.float32)
    combine = jnp.where(chosen, spread(weight, CAP, lax.Precision.HIGHEST), 0.0)
    mixed = jnp.dot(
        combine, returned, precision=lax.Precision.HIGHEST, preferred_element_type=jnp.float32
    )
    return mixed.astype(jnp.bfloat16)


def mapped(mesh):
    finer = Mesh(mesh.devices.reshape(-1, 2, 2, 2, 4), EP_TP)
    placed = (
        P(EP, None),
        P(),
        P(EP, None),
        P(EP, None),
        P(None, EP_TP),
        P(None, EP_TP),
        P(EP, "y"),
    )
    return jax.shard_map(layer, mesh=finer, in_specs=placed, out_specs=P(EP, "y"), check_vma=False)


def solution(mesh):
    return mapped(mesh)
```

```python
import jax
import jax.numpy as jnp
from jax import lax
from jax.experimental import pallas as pl
from jax.experimental.pallas import tpu as pltpu
from jax.sharding import Mesh
from jax.sharding import PartitionSpec as P


EPS = 1e-06
EP = ("z", "xh", "xl", "c")
EP_TP = ("z", "xh", "xl", "c", "y")
CAP = 12
SWAP = [(0, 1), (1, 0)]


def rms_rows(values, gain):
    widened = values.astype(jnp.float32)
    scale = lax.rsqrt(jnp.mean(widened * widened, axis=-1, keepdims=True) + EPS)
    return (widened * scale * gain).astype(jnp.bfloat16)


def shift(block, by):
    return lax.ppermute(block, "y", [(y, (y + by) % 4) for y in range(4)])


def around(block, by):
    pairs = [(y, (y + by) % 4) for y in range(4)] + [(4 + y, 4 + (y - by) % 4) for y in range(4)]
    return lax.ppermute(block, ("c", "y"), pairs)


def swap(block, axis):
    return lax.ppermute(block, axis, SWAP)


def dot32(a, b):
    return jnp.dot(a, b, preferred_element_type=jnp.float32)


def spread(per_expert, width, precision=None):
    count = per_expert.shape[1]
    expert = lax.broadcasted_iota(jnp.int32, (count, count * width), 1) // width
    own = lax.broadcasted_iota(jnp.int32, (count, count * width), 0)
    table = (expert == own).astype(per_expert.dtype)
    return jnp.dot(per_expert, table, precision=precision, preferred_element_type=jnp.float32)


def expert_kernel(at_ref, *refs):
    blocks, gates, uppers, downs = refs[0:4], refs[4:8], refs[8:12], refs[12:16]
    hidden_ref, part_ref, rows, wide, tall, sems, row_sems = refs[16:]
    depth = wide.shape[2] // 2
    count = blocks[0].shape[0]
    moves, copies = [], []
    for i, ahead in enumerate((0, -at_ref[1], 2, at_ref[1])):
        place = pl.ds(pl.multiple_of(((at_ref[0] + ahead) & 3) * count, 16), count)
        moves.append(pltpu.make_async_copy(blocks[i], rows.at[place], row_sems.at[i]))
    for i in range(4):
        gate_at, up_at = wide.at[i, :, pl.ds(0, depth)], wide.at[i, :, pl.ds(depth, depth)]
        copies.append(pltpu.make_async_copy(gates[i], gate_at, sems.at[3 * i]))
        copies.append(pltpu.make_async_copy(uppers[i], up_at, sems.at[3 * i + 1]))
        copies.append(pltpu.make_async_copy(downs[i], tall.at[i], sems.at[3 * i + 2]))
    for copy in moves + copies:
        copy.start()
    for move in moves:
        move.wait()
    total = jnp.zeros(part_ref.shape, jnp.float32)
    for i in range(4):
        copies[3 * i].wait()
        copies[3 * i + 1].wait()
        both = dot32(rows[...], wide[i])
        piece = (jax.nn.silu(both[:, :depth]) * both[:, depth:]).astype(jnp.bfloat16)
        hidden_ref[:, i * depth : (i + 1) * depth] = piece
        copies[3 * i + 2].wait()
        total += dot32(piece, tall[i])
    part_ref[...] = total.astype(part_ref.dtype)


def run_experts(at, blocks, gates, uppers, downs):
    count, width = 4 * blocks[0].shape[0], blocks[0].shape[1]
    depth = gates[0].shape[1]
    out_width = downs[0].shape[1]
    return pl.pallas_call(
        expert_kernel,
        in_specs=[pl.BlockSpec(memory_space=pltpu.SMEM)]
        + [pl.BlockSpec(memory_space=pl.ANY)] * 16,
        out_specs=[pl.BlockSpec(memory_space=pltpu.VMEM)] * 2,
        out_shape=[
            jax.ShapeDtypeStruct((count, 4 * depth), jnp.bfloat16),
            jax.ShapeDtypeStruct((count, out_width), jnp.bfloat16),
        ],
        scratch_shapes=[
            pltpu.VMEM((count, width), jnp.bfloat16),
            pltpu.VMEM((4, width, 2 * depth), jnp.bfloat16),
            pltpu.VMEM((4, depth, out_width), jnp.bfloat16),
            pltpu.SemaphoreType.DMA((12,)),
            pltpu.SemaphoreType.DMA((4,)),
        ],
        cost_estimate=pl.CostEstimate(
            flops=16 * count * width * depth,
            bytes_accessed=16 * width * depth,
            transcendentals=4 * count * depth,
        ),
        compiler_params=pltpu.CompilerParams(vmem_limit_bytes=20 << 20),
        name="experts",
    )(at, *blocks, *gates, *uppers, *downs)


def down_kernel(pick_ref, hidden_ref, *refs):
    downs, outs, (tall, sems) = refs[:4], refs[4:-2], refs[-2:]
    depth = tall.shape[1]
    copies = [
        pltpu.make_async_copy(downs[i].at[pick_ref[n]], tall.at[4 * n + i], sems.at[4 * n + i])
        for n in range(len(outs))
        for i in range(4)
    ]
    for copy in copies:
        copy.start()
    for n, out in enumerate(outs):
        total = jnp.zeros(out.shape, jnp.float32)
        for i in range(4):
            copies[4 * n + i].wait()
            total += dot32(hidden_ref[:, i * depth : (i + 1) * depth], tall[4 * n + i])
        out[...] = total.astype(out.dtype)


def run_down(picks, hidden, downs, dtypes):
    count, parts = hidden.shape[0], len(dtypes)
    _, depth, out_width = downs[0].shape
    return pl.pallas_call(
        down_kernel,
        in_specs=[pl.BlockSpec(memory_space=pltpu.SMEM), pl.BlockSpec(memory_space=pltpu.VMEM)]
        + [pl.BlockSpec(memory_space=pl.ANY)] * 4,
        out_specs=[pl.BlockSpec(memory_space=pltpu.VMEM)] * parts,
        out_shape=[jax.ShapeDtypeStruct((count, out_width), dtype) for dtype in dtypes],
        scratch_shapes=[
            pltpu.VMEM((4 * parts, depth, out_width), jnp.bfloat16),
            pltpu.SemaphoreType.DMA((4 * parts,)),
        ],
        cost_estimate=pl.CostEstimate(
            flops=8 * parts * count * depth * out_width,
            bytes_accessed=8 * parts * depth * out_width,
            transcendentals=0,
        ),
        compiler_params=pltpu.CompilerParams(vmem_limit_bytes=12 << 20),
        name="down",
    )(picks, hidden, *downs)


def layer(tokens, norm_gain, expert_ids, gate_weights, w_gate, w_up, w_down):
    y = lax.axis_index("y")
    rows = tokens.shape[0]
    width = tokens.shape[1]
    share = CAP // 4
    expert_count = lax.axis_size(("z", "xh"))
    block_rows = expert_count * share
    depth = w_gate.shape[1]
    out_width = w_down.shape[1]

    gate_x = swap(w_gate, "xl")
    up_x = swap(w_up, "xl")

    normed = rms_rows(tokens, norm_gain)
    experts = jnp.arange(expert_count, dtype=jnp.int32)[None, :]
    first = expert_ids[:, 0:1] == experts
    second = expert_ids[:, 1:2] == experts
    named = first | second
    weight = jnp.where(first, gate_weights[:, 0:1], 0.0) + jnp.where(
        second, gate_weights[:, 1:2], 0.0
    )
    earlier = (
        lax.broadcasted_iota(jnp.int32, (rows, rows), 0)
        > lax.broadcasted_iota(jnp.int32, (rows, rows), 1)
    ).astype(jnp.bfloat16)
    rank = dot32(earlier, named.astype(jnp.bfloat16))
    rank = jnp.where(named, rank, -1.0).astype(jnp.bfloat16)
    column = lax.broadcasted_iota(jnp.int32, (1, block_rows), 1)
    slot = share * y + column % share
    selector = (spread(rank, share) == slot.astype(jnp.float32)).astype(jnp.bfloat16)
    mine = lax.dot_general(
        selector, normed, (((0,), (0,)), ((), ())), preferred_element_type=jnp.float32
    ).astype(jnp.bfloat16)
    mine = mine.reshape(expert_count, share * width // 128, 128)
    arrived = lax.all_to_all(mine, ("z", "xh"), 0, 0, tiled=True)
    near = arrived.reshape(block_rows, width)

    cut = []
    for k in range(4):
        start = ((y - k) & 3) * depth
        cut.append(lax.dynamic_slice_in_dim(w_down, start, depth, 0))
    for k in (2, 1, 3):
        cut[k] = shift(cut[k], -k)
    gate_c = swap(w_gate, "c")
    up_c = swap(w_up, "c")
    leads = [cut[2], swap(cut[2], "c"), swap(cut[2], "xl")]
    leads.append(swap(leads[2], "c"))
    rest = jnp.stack([cut[1], cut[3], cut[0]])
    rests = [rest, swap(rest, "c"), swap(rest, "xl")]
    rests.append(swap(rests[2], "c"))
    gate_d = swap(gate_x, "c")
    up_d = swap(up_x, "c")

    core = lax.axis_index("c").astype(jnp.int32)
    ahead = around(near, 1)
    behind = around(near, -1)
    across = around(ahead, 1)
    blocks = (near, ahead, across, behind)
    gates, uppers = (w_gate, gate_c, gate_x, gate_d), (w_up, up_c, up_x, up_d)
    at = jnp.stack([y.astype(jnp.int32), 1 - 2 * core])
    hidden, away = run_experts(at, blocks, gates, uppers, leads)
    middle = around(away, 1)
    against, along = run_down(
        jnp.stack([1 - core, core]), hidden, rests, (jnp.bfloat16, jnp.float32)
    )
    first = around(against, -1)
    second = around((along + middle.astype(jnp.float32)).astype(jnp.bfloat16), 1)
    (total,) = run_down(jnp.full((1,), 2, jnp.int32), hidden, rests, (jnp.float32,))
    total = total + first.astype(jnp.float32) + second.astype(jnp.float32)
    home = total.astype(jnp.bfloat16)
    home = home.reshape(4, expert_count, share, out_width).transpose(1, 0, 2, 3)
    home = home.reshape(expert_count, CAP * out_width // 128, 128)
    returned = lax.all_to_all(home, ("z", "xh"), 0, 0, tiled=True)
    returned = returned.reshape(expert_count * CAP, out_width).astype(jnp.float32)
    column = lax.broadcasted_iota(jnp.int32, (1, expert_count * CAP), 1) % CAP
    chosen = spread(rank, CAP) == column.astype(jnp.float32)
    combine = jnp.where(chosen, spread(weight, CAP, lax.Precision.HIGHEST), 0.0)
    mixed = jnp.dot(
        combine, returned, precision=lax.Precision.HIGHEST, preferred_element_type=jnp.float32
    )
    return mixed.astype(jnp.bfloat16)


def mapped(mesh):
    finer = Mesh(mesh.devices.reshape(-1, 2, 2, 2, 4), EP_TP)
    placed = (
        P(EP, None),
        P(),
        P(EP, None),
        P(EP, None),
        P(None, EP_TP),
        P(None, EP_TP),
        P(EP, "y"),
    )
    return jax.shard_map(layer, mesh=finer, in_specs=placed, out_specs=P(EP, "y"), check_vma=False)


def solution(mesh):
    return mapped(mesh)
```

```python
import functools

import jax
import jax.numpy as jnp
from jax import lax
from jax.experimental import pallas as pl
from jax.experimental.pallas import tpu as pltpu
from jax.sharding import Mesh
from jax.sharding import PartitionSpec as P


EPS = 1e-06
EP = ("z", "xh", "xl", "c")
EP_TP = ("z", "xh", "xl", "c", "y")
CAP = 12
SWAP = [(0, 1), (1, 0)]


def rms_rows(values, gain):
    widened = values.astype(jnp.float32)
    scale = lax.rsqrt(jnp.mean(widened * widened, axis=-1, keepdims=True) + EPS)
    return (widened * scale * gain).astype(jnp.bfloat16)


def shift(block, by):
    return lax.ppermute(block, "y", [(y, (y + by) % 4) for y in range(4)])


def around(block, by):
    pairs = [(y, (y + by) % 4) for y in range(4)] + [(4 + y, 4 + (y - by) % 4) for y in range(4)]
    return lax.ppermute(block, ("c", "y"), pairs)


def swap(block, axis):
    return lax.ppermute(block, axis, SWAP)


def dot32(a, b):
    return jnp.dot(a, b, preferred_element_type=jnp.float32)


def spread(per_expert, width, precision=None):
    count = per_expert.shape[1]
    expert = lax.broadcasted_iota(jnp.int32, (count, count * width), 1) // width
    own = lax.broadcasted_iota(jnp.int32, (count, count * width), 0)
    table = (expert == own).astype(per_expert.dtype)
    return jnp.dot(per_expert, table, precision=precision, preferred_element_type=jnp.float32)


def expert_kernel(at_ref, *refs):
    blocks, gates, uppers, downs = refs[0:4], refs[4:8], refs[8:12], refs[12:16]
    hidden_ref, part_ref, rows, wide, tall, sems, row_sems = refs[16:]
    depth = wide.shape[2] // 2
    count = blocks[0].shape[0]
    moves, copies = [], []
    for i in range(4):
        place = pl.ds(pl.multiple_of(((at_ref[0] + i) & 3) * count, 16), count)
        moves.append(pltpu.make_async_copy(blocks[i], rows.at[place], row_sems.at[i]))
    for i in range(4):
        gate_at, up_at = wide.at[i, :, pl.ds(0, depth)], wide.at[i, :, pl.ds(depth, depth)]
        copies.append(pltpu.make_async_copy(gates[i], gate_at, sems.at[3 * i]))
        copies.append(pltpu.make_async_copy(uppers[i], up_at, sems.at[3 * i + 1]))
        copies.append(pltpu.make_async_copy(downs[i], tall.at[i], sems.at[3 * i + 2]))
    for copy in moves + copies:
        copy.start()
    for move in moves:
        move.wait()
    total = jnp.zeros(part_ref.shape, jnp.float32)
    for i in range(4):
        copies[3 * i].wait()
        copies[3 * i + 1].wait()
        both = dot32(rows[...], wide[i])
        piece = (jax.nn.silu(both[:, :depth]) * both[:, depth:]).astype(jnp.bfloat16)
        hidden_ref[:, i * depth : (i + 1) * depth] = piece
        copies[3 * i + 2].wait()
        total += dot32(piece, tall[i])
    part_ref[...] = total.astype(part_ref.dtype)


def run_experts(at, blocks, gates, uppers, downs):
    count, width = 4 * blocks[0].shape[0], blocks[0].shape[1]
    depth = gates[0].shape[1]
    out_width = downs[0].shape[1]
    return pl.pallas_call(
        expert_kernel,
        in_specs=[pl.BlockSpec(memory_space=pltpu.SMEM)]
        + [pl.BlockSpec(memory_space=pl.ANY)] * 16,
        out_specs=[pl.BlockSpec(memory_space=pltpu.VMEM)] * 2,
        out_shape=[
            jax.ShapeDtypeStruct((count, 4 * depth), jnp.bfloat16),
            jax.ShapeDtypeStruct((count, out_width), jnp.bfloat16),
        ],
        scratch_shapes=[
            pltpu.VMEM((count, width), jnp.bfloat16),
            pltpu.VMEM((4, width, 2 * depth), jnp.bfloat16),
            pltpu.VMEM((4, depth, out_width), jnp.bfloat16),
            pltpu.SemaphoreType.DMA((12,)),
            pltpu.SemaphoreType.DMA((4,)),
        ],
        cost_estimate=pl.CostEstimate(
            flops=16 * count * width * depth,
            bytes_accessed=16 * width * depth,
            transcendentals=4 * count * depth,
        ),
        compiler_params=pltpu.CompilerParams(vmem_limit_bytes=20 << 20),
        name="experts",
    )(at, *blocks, *gates, *uppers, *downs)


def down_kernel(fixed, core_ref, hidden_ref, *refs):
    downs, outs, (tall, sems) = refs[:4], refs[4:-2], refs[-2:]
    depth = tall.shape[1]
    picks = fixed or (1 - core_ref[0], core_ref[0])
    copies = [
        pltpu.make_async_copy(downs[i].at[picks[n]], tall.at[4 * n + i], sems.at[4 * n + i])
        for n in range(len(outs))
        for i in range(4)
    ]
    for copy in copies:
        copy.start()
    for n, out in enumerate(outs):
        total = jnp.zeros(out.shape, jnp.float32)
        for i in range(4):
            copies[4 * n + i].wait()
            total += dot32(hidden_ref[:, i * depth : (i + 1) * depth], tall[4 * n + i])
        out[...] = total.astype(out.dtype)


def run_down(fixed, core, hidden, downs, dtypes):
    count, parts = hidden.shape[0], len(dtypes)
    _, depth, out_width = downs[0].shape
    return pl.pallas_call(
        functools.partial(down_kernel, fixed),
        in_specs=[pl.BlockSpec(memory_space=pltpu.SMEM), pl.BlockSpec(memory_space=pltpu.VMEM)]
        + [pl.BlockSpec(memory_space=pl.ANY)] * 4,
        out_specs=[pl.BlockSpec(memory_space=pltpu.VMEM)] * parts,
        out_shape=[jax.ShapeDtypeStruct((count, out_width), dtype) for dtype in dtypes],
        scratch_shapes=[
            pltpu.VMEM((4 * parts, depth, out_width), jnp.bfloat16),
            pltpu.SemaphoreType.DMA((4 * parts,)),
        ],
        cost_estimate=pl.CostEstimate(
            flops=8 * parts * count * depth * out_width,
            bytes_accessed=8 * parts * depth * out_width,
            transcendentals=0,
        ),
        compiler_params=pltpu.CompilerParams(vmem_limit_bytes=12 << 20),
        name="down",
    )(core, hidden, *downs)


def layer(tokens, norm_gain, expert_ids, gate_weights, w_gate, w_up, w_down):
    y = lax.axis_index("y")
    rows = tokens.shape[0]
    width = tokens.shape[1]
    share = CAP // 4
    expert_count = lax.axis_size(("z", "xh"))
    block_rows = expert_count * share
    depth = w_gate.shape[1]
    out_width = w_down.shape[1]

    gate_x = swap(w_gate, "xl")
    up_x = swap(w_up, "xl")

    normed = rms_rows(tokens, norm_gain)
    experts = jnp.arange(expert_count, dtype=jnp.int32)[None, :]
    first = expert_ids[:, 0:1] == experts
    second = expert_ids[:, 1:2] == experts
    named = first | second
    weight = jnp.where(first, gate_weights[:, 0:1], 0.0) + jnp.where(
        second, gate_weights[:, 1:2], 0.0
    )
    earlier = (
        lax.broadcasted_iota(jnp.int32, (rows, rows), 0)
        > lax.broadcasted_iota(jnp.int32, (rows, rows), 1)
    ).astype(jnp.bfloat16)
    rank = dot32(earlier, named.astype(jnp.bfloat16))
    rank = jnp.where(named, rank, -1.0).astype(jnp.bfloat16)
    column = lax.broadcasted_iota(jnp.int32, (1, block_rows), 1)
    slot = share * y + column % share
    selector = (spread(rank, share) == slot.astype(jnp.float32)).astype(jnp.bfloat16)
    mine = lax.dot_general(
        selector, normed, (((0,), (0,)), ((), ())), preferred_element_type=jnp.float32
    ).astype(jnp.bfloat16)
    mine = mine.reshape(expert_count, share * width // 128, 128)
    arrived = lax.all_to_all(mine, ("z", "xh"), 0, 0, tiled=True)
    near = arrived.reshape(block_rows, width)

    cut = []
    for k in range(4):
        start = ((y - k) & 3) * depth
        cut.append(lax.dynamic_slice_in_dim(w_down, start, depth, 0))
    for k in (2, 1, 3):
        cut[k] = shift(cut[k], -k)
    gate_c = swap(w_gate, "c")
    up_c = swap(w_up, "c")
    leads = [cut[2], swap(cut[2], "c"), swap(cut[2], "xl")]
    leads.append(swap(leads[2], "c"))
    rest = jnp.stack([cut[1], cut[3], cut[0]])
    rests = [rest, swap(rest, "c"), swap(rest, "xl")]
    rests.append(swap(rests[2], "c"))
    gate_d = swap(gate_x, "c")
    up_d = swap(up_x, "c")

    lower_core = lax.axis_index("c") == 0
    below = shift(near, 1)
    above = shift(near, -1)
    across = around(jnp.where(lower_core, below, above), 1)
    blocks = (near, above, across, below)
    gates, uppers = (w_gate, gate_c, gate_x, gate_d), (w_up, up_c, up_x, up_d)
    hidden, away = run_experts(y[None].astype(jnp.int32), blocks, gates, uppers, leads)
    middle = around(away, 1)
    core = lax.axis_index("c").astype(jnp.int32)[None]
    against, along = run_down((), core, hidden, rests, (jnp.bfloat16, jnp.float32))
    first = around(against, -1)
    second = around((along + middle.astype(jnp.float32)).astype(jnp.bfloat16), 1)
    (total,) = run_down((2,), core, hidden, rests, (jnp.float32,))
    total = total + first.astype(jnp.float32) + second.astype(jnp.float32)
    home = total.astype(jnp.bfloat16)
    home = home.reshape(4, expert_count, share, out_width).transpose(1, 0, 2, 3)
    home = home.reshape(expert_count, CAP * out_width // 128, 128)
    returned = lax.all_to_all(home, ("z", "xh"), 0, 0, tiled=True)
    returned = returned.reshape(expert_count * CAP, out_width).astype(jnp.float32)
    column = lax.broadcasted_iota(jnp.int32, (1, expert_count * CAP), 1) % CAP
    chosen = spread(rank, CAP) == column.astype(jnp.float32)
    combine = jnp.where(chosen, spread(weight, CAP, lax.Precision.HIGHEST), 0.0)
    mixed = jnp.dot(
        combine, returned, precision=lax.Precision.HIGHEST, preferred_element_type=jnp.float32
    )
    return mixed.astype(jnp.bfloat16)


def mapped(mesh):
    finer = Mesh(mesh.devices.reshape(-1, 2, 2, 2, 4), EP_TP)
    placed = (
        P(EP, None),
        P(),
        P(EP, None),
        P(EP, None),
        P(None, EP_TP),
        P(None, EP_TP),
        P(EP, "y"),
    )
    return jax.shard_map(layer, mesh=finer, in_specs=placed, out_specs=P(EP, "y"), check_vma=False)


def solution(mesh):
    return mapped(mesh)
```
